32 devices in a mesh: sp: 8 (over z, x), tp: 4 (over y, core).
Axes of the slice: x: 2, y: 2, z: 4, core: 2. Of those that a mesh axis runs over, the one named last changes fastest.
Arguments:
- stream: bfloat16 [2048, 2048], P(('sp', 'tp')), may hold values from -6 to 6
- query_a: bfloat16 [2048, 384], P('sp', 'tp'), may hold values from -400 to 400
- query_b: bfloat16 [2048, 640], P('sp', 'tp'), may hold values from -400 to 400
- latent: bfloat16 [2048, 256], P('sp'), may hold values from -6 to 6
- rotary_key: bfloat16 [2048, 32], P('sp'), may hold values from -6 to 6
- latent_gain: float32 [256], replicated, may hold values from 0.1 to 1.9
- key_gain_a: float32 [96], replicated, may hold values from 0.1 to 1.9
- key_gain_b: float32 [160], replicated, may hold values from 0.1 to 1.9
- w_key_a: bfloat16 [256, 256], P(None, 'tp'), may hold values from -0.375 to 0.375
- w_value_a: bfloat16 [256, 256], P(None, 'tp'), may hold values from -0.375 to 0.375
- w_key_b: bfloat16 [256, 512], P(None, 'tp'), may hold values from -0.375 to 0.375
- w_value_b: bfloat16 [256, 512], P(None, 'tp'), may hold values from -0.375 to 0.375
- w_out_a: bfloat16 [256, 2048], P('tp'), may hold values from -0.21875 to 0.21875
- w_out_b: bfloat16 [512, 2048], P('tp'), may hold values from -0.21875 to 0.21875
- norm_gain: float32 [2048], replicated, may hold values from 0.1 to 1.9
- w_up: bfloat16 [2048, 4096], P('sp', 'tp'), may hold values from -0.125 to 0.125
- w_down: bfloat16 [4096, 2048], P('tp', 'sp'), may hold values from -0.09375 to 0.09375
Outputs:
- result: bfloat16 [2048, 2048], P(('sp', 'tp'))
The draws below stay inside these ranges and needn't reach their ends.
All inputs are finite; a program needn't handle non-finite values.
Results may differ from the reference program's by a relative error of at most 0.018.
The reference program's roundings to bfloat16 on the way count: a program that leaves them out, or rounds other values in their place, can miss the bound.
Values may be sent and summed in bfloat16 or wider, within the bound.
A program may use at most 128 MiB of HBM per device.

```python
import math
import jax
import jax.numpy as jnp
from jax import lax

D = 2048
HEADS_A = 4
HEADS_B = 4
NOPE_A = 64
V_A = 64
NOPE_B = 128
V_B = 128
ROPE = 32
KV_RANK = 256
FF = 4096
TOKENS = 2048


def scaled_rows(key, count, width):
    base_key = jax.random.fold_in(key, 0)
    base = jax.random.normal(base_key, (count, width), jnp.float32)
    factor = 2.5 * jnp.ones((count, 1), jnp.float32)
    return jnp.clip(base * factor, -400.0, 400.0)


def draw_query_a(key, part):
    return scaled_rows(jax.random.fold_in(key, 11), TOKENS, HEADS_A * (NOPE_A + ROPE)).astype(jnp.bfloat16)


def draw_query_b(key, part):
    return scaled_rows(jax.random.fold_in(key, 23), TOKENS, HEADS_B * (NOPE_B + ROPE)).astype(jnp.bfloat16)


def block_scale(stream_key, shape, shards, smallest, largest):
    level = 1.0
    for position, blocks in shards:
        heights = jax.random.uniform(jax.random.fold_in(jax.random.fold_in(stream_key, 6), position), (blocks,), jnp.float32, smallest / len(shards), largest / len(shards))
        level = level * jnp.repeat(jnp.exp(heights), shape[position] // blocks).reshape((-1,) + (1,) * (len(shape) - 1 - position))
    return level


def scatter_about(own_key, shape, scale, reach, cuts=(), kind=jnp.bfloat16):
    array = scale * jax.random.normal(own_key, shape, jnp.float32)
    if cuts:
        array = array * block_scale(own_key, shape, cuts, -0.22, 0.18)
    return jnp.clip(array, -reach, reach).astype(kind)


def setup_inputs(seed: int = 0) -> dict:
    splits = jax.random.split(jax.random.key(seed), 18)
    stream = scatter_about(splits[0], (TOKENS, D), 0.4, 6.0, ((0, 32),))
    query_a = draw_query_a(jax.random.fold_in(splits[17], 71), 0)
    query_b = draw_query_b(jax.random.fold_in(splits[17], 71), 0)
    latent = scatter_about(splits[3], (TOKENS, KV_RANK), 1.0, 6.0, ((0, 8),))
    rotary_key = scatter_about(splits[4], (TOKENS, ROPE), 1.0, 6.0, ((0, 8),))
    latent_gain = jnp.clip(1.0 + 0.18 * jax.random.normal(splits[5], (KV_RANK,), jnp.float32), 0.1, 1.9)
    key_gain_a = jnp.clip(1.0 + 0.18 * jax.random.normal(splits[6], (NOPE_A + ROPE,), jnp.float32), 0.1, 1.9)
    key_gain_b = jnp.clip(1.0 + 0.18 * jax.random.normal(splits[7], (NOPE_B + ROPE,), jnp.float32), 0.1, 1.9)
    w_key_a = scatter_about(splits[8], (KV_RANK, HEADS_A * NOPE_A), KV_RANK ** -0.5, 0.375, ((1, 4),))
    w_value_a = scatter_about(splits[9], (KV_RANK, HEADS_A * V_A), KV_RANK ** -0.5, 0.375, ((1, 4),))
    w_key_b = scatter_about(splits[10], (KV_RANK, HEADS_B * NOPE_B), KV_RANK ** -0.5, 0.375, ((1, 4),))
    w_value_b = scatter_about(splits[11], (KV_RANK, HEADS_B * V_B), KV_RANK ** -0.5, 0.375, ((1, 4),))
    w_out_a = scatter_about(splits[12], (HEADS_A * V_A, D), (HEADS_A * V_A + HEADS_B * V_B) ** -0.5, 0.21875, ((0, 4),))
    w_out_b = scatter_about(splits[13], (HEADS_B * V_B, D), (HEADS_A * V_A + HEADS_B * V_B) ** -0.5, 0.21875, ((0, 4),))
    norm_gain = jnp.clip(1.0 + 0.18 * jax.random.normal(splits[14], (D,), jnp.float32), 0.1, 1.9)
    w_up = scatter_about(splits[15], (D, FF), D ** -0.5, 0.125, ((0, 8), (1, 4)))
    w_down = scatter_about(splits[16], (FF, D), FF ** -0.5, 0.09375, ((0, 4), (1, 8)))
    return {"stream": stream, "query_a": query_a, "query_b": query_b, "latent": latent, "rotary_key": rotary_key, "latent_gain": latent_gain, "key_gain_a": key_gain_a, "key_gain_b": key_gain_b, "w_key_a": w_key_a, "w_value_a": w_value_a, "w_key_b": w_key_b, "w_value_b": w_value_b, "w_out_a": w_out_a, "w_out_b": w_out_b, "norm_gain": norm_gain, "w_up": w_up, "w_down": w_down}


EPSILON = 1e-06
THETA = 10000.0

def rms_scale(values, gain):
    wide = values.astype(jnp.float32)
    return wide * lax.rsqrt(lax.optimization_barrier(jnp.mean(wide * wide, axis=-1, keepdims=True)) + EPSILON) * gain.astype(jnp.float32)

def rotate(tail, positions):
    half = tail.shape[-1] // 2
    freqs = THETA ** (-jnp.arange(half, dtype=jnp.float32) / half)
    angle = positions[:, None, None] * freqs
    cosine = jnp.cos(angle)
    sine = jnp.sin(angle)
    first = tail[..., :half]
    second = tail[..., half:]
    return jnp.concatenate([first * cosine - second * sine, second * cosine + first * sine], axis=-1)

def make_keys(normed, rotary_key, w_key, w_value, key_gain, nope, positions):
    count = normed.shape[0]
    heads = w_key.shape[1] // nope
    head_nope = jnp.dot(normed, w_key, preferred_element_type=jnp.float32).astype(jnp.bfloat16)
    head_nope = head_nope.reshape(count, heads, nope)
    values = jnp.dot(normed, w_value, preferred_element_type=jnp.float32).astype(jnp.bfloat16)
    shared = jnp.broadcast_to(rotary_key[:, None, :], (count, heads, rotary_key.shape[1]))
    joined = rms_scale(jnp.concatenate([head_nope, shared], axis=-1), key_gain)
    turned = rotate(joined[..., nope:], positions)
    keys_out = jnp.concatenate([joined[..., :nope], turned], axis=-1).astype(jnp.bfloat16)
    return (keys_out.reshape(count, -1), values)

def attention(queries, keys_in, values_in, depth):
    total_rows = keys_in.shape[0]
    heads = keys_in.shape[1] // depth
    key_view = keys_in.astype(jnp.float32).reshape(total_rows, heads, depth)
    value_view = values_in.astype(jnp.float32).reshape(total_rows, heads, -1)
    block = math.gcd(queries.shape[0], 512)
    blocks = queries.astype(jnp.float32).reshape(-1, block, heads, depth)

    def one_block(block_queries):
        scores = jnp.einsum('qhd,khd->qhk', block_queries, key_view) * depth ** (-0.5)
        peak = lax.optimization_barrier(jnp.max(scores, axis=-1))
        shifted = jnp.exp(scores - peak[..., None])
        totals = lax.optimization_barrier(jnp.sum(shifted, axis=-1))
        weights = lax.optimization_barrier(shifted.astype(jnp.bfloat16)).astype(jnp.float32)
        weighted = jnp.einsum('qhk,khd->qhd', weights, value_view)
        return (weighted / totals[..., None]).astype(jnp.bfloat16).reshape(block, -1)
    return lax.map(one_block, blocks).reshape(queries.shape[0], -1)

def reference(stream, query_a, query_b, latent, rotary_key, latent_gain, key_gain_a, key_gain_b, w_key_a, w_value_a, w_key_b, w_value_b, w_out_a, w_out_b, norm_gain, w_up, w_down):
    positions = jnp.arange(TOKENS).astype(jnp.float32)
    normed_latent = rms_scale(latent, latent_gain).astype(jnp.bfloat16)
    key_a, value_a = make_keys(normed_latent, rotary_key, w_key_a, w_value_a, key_gain_a, NOPE_A, positions)
    key_b, value_b = make_keys(normed_latent, rotary_key, w_key_b, w_value_b, key_gain_b, NOPE_B, positions)
    attended_a = attention(query_a, key_a, value_a, NOPE_A + ROPE)
    attended_b = attention(query_b, key_b, value_b, NOPE_B + ROPE)
    mixed = jnp.dot(attended_a, w_out_a, preferred_element_type=jnp.float32) + jnp.dot(attended_b, w_out_b, preferred_element_type=jnp.float32)
    residual = (stream.astype(jnp.float32) + mixed).astype(jnp.bfloat16)
    normed = rms_scale(residual, norm_gain).astype(jnp.bfloat16)
    activated = jnp.square(jax.nn.relu(jnp.dot(normed, w_up, preferred_element_type=jnp.float32))).astype(jnp.bfloat16)
    summed = jnp.dot(activated, w_down, preferred_element_type=jnp.float32)
    return (residual.astype(jnp.float32) + summed).astype(jnp.bfloat16)
```

```python
import functools

import jax
import jax.numpy as jnp
import numpy as np
from jax import lax
from jax.experimental import pallas as pl
from jax.experimental.pallas import tpu as pltpu
from jax.sharding import PartitionSpec as P

NOPE_A = 64
V_A = 64
NOPE_B = 128
V_B = 128
ROPE = 32

EPSILON = 1e-06
THETA = 10000.0
F32 = jnp.float32
BF16 = jnp.bfloat16


def kernel(
    n, m,
    stream, q_a, q_b, latent, rotary_t, table_h, lat_gain, gain_a, gain_b,
    wk_a, wv_a, wk_b, wv_b, wo_a, wo_b, norm_gain, w_up, w_down,
    out,
    lat, key_a, key_b, val_a, val_b, att, rows, goa, gob,
    gup, gdown, x, hid, act, res, even, odd, sib, part, land, table,
    lat_s, lat_r, latz_s, latf_s, latf_r, oa_s, oa_r, ob_s, ob_r,
    up_s, up_r, dn_s, dn_r, at_s, at_r, x_s, x_r, rs_s, rs_r, loc,
):
    s = lax.axis_index("sp")
    t = lax.axis_index("tp")
    core = t & 1
    length = q_a.shape[1]
    own = stream.shape[0]
    prow = lat.shape[1]
    half_rows = prow // 2
    depth_a = NOPE_A + ROPE
    depth_b = NOPE_B + ROPE
    heads_a = wk_a.shape[0] // NOPE_A
    heads_b = wk_b.shape[1] // NOPE_B
    hidden = gup.shape[2]
    wrows = w_up.shape[0]
    wcols = w_down.shape[1]
    features = stream.shape[1]
    width_a = heads_a * V_A
    width_b = heads_b * V_B
    start_b = att.shape[2] - width_b
    quarter = n // 4
    per = n // 8
    zone = s // quarter
    inner = (zone ^ (zone // 2)) & 1
    near = list(range(2, 2 * quarter, 2))
    first_far = (2 + inner) * quarter
    last_far = (3 - inner) * quarter
    up_half = wrows // 2
    cuts = 2 if wcols % 256 == 0 else 1
    cut = wcols // cuts

    def every(start, fn):
        if per == 1:
            fn(start)
        else:
            def step(j, carry):
                fn(start + 2 * j)
                return carry
            lax.fori_loop(0, per, step, 0)

    def copy(src, dst, ssem, rsem, sp, tp):
        return pltpu.make_async_remote_copy(
            src_ref=src, dst_ref=dst, send_sem=ssem, recv_sem=rsem,
            device_id={"sp": sp, "tp": tp}, device_id_type=pl.DeviceIdType.MESH,
        )

    barrier = pltpu.get_barrier_semaphore()

    def greet(sp, tp):
        pl.semaphore_signal(barrier, inc=1, device_id={"sp": sp, "tp": tp},
                            device_id_type=pl.DeviceIdType.MESH)

    for k in range(1, n):
        greet(s ^ k, t)
    for k in range(1, m):
        greet(s, t ^ k)
    greet(s ^ 2, t ^ 2)

    def halves(target):
        return pl.ds(pl.multiple_of(((target // 2) % 2) * hidden, 128), hidden)

    locals_ = [
        pltpu.make_async_copy(latent, lat.at[0, pl.ds(0, length)], loc.at[0]),
        pltpu.make_async_copy(rotary_t, lat.at[0, pl.ds(length, prow - length)], loc.at[1]),
        pltpu.make_async_copy(table_h, table, loc.at[2]),
        pltpu.make_async_copy(w_up.at[:, halves(s)], gup.at[0], loc.at[3]),
        pltpu.make_async_copy(w_down.at[halves(s)], gdown.at[0], loc.at[4]),
    ]
    for c in locals_:
        c.start()
    locals_[0].wait()
    locals_[1].wait()
    pl.semaphore_wait(barrier, n + m - 1)

    mine = pl.ds(pl.multiple_of(core * half_rows, 16), half_rows)
    other = pl.ds(pl.multiple_of((1 - core) * half_rows, 16), half_rows)

    def lat_direct(k):
        return copy(lat.at[0, mine], lat.at[k, mine], lat_s.at[k], lat_r.at[k], s ^ k, t)

    def lat_across(k):
        return copy(lat.at[k, mine], lat.at[k + 1, mine], lat_s.at[k + 1], lat_r.at[k + 1], s ^ 1, t)

    def lat_along(k):
        j = k ^ quarter
        return copy(lat.at[k, mine], lat.at[j, mine], latz_s.at[k], lat_r.at[j], s ^ quarter, t)

    def lat_sibling(k):
        return copy(lat.at[k, mine], lat.at[k, mine], latf_s.at[k], latf_r.at[k], s, t ^ 1)

    def up_piece(k, r):
        at = pl.ds(r * up_half, up_half)
        return copy(w_up.at[at, halves(s ^ k)], gup.at[k, at], up_s.at[2 * k + r],
                    up_r.at[2 * k + r], s ^ k, t)

    def up_across(k, r):
        at = pl.ds(r * up_half, up_half)
        return copy(gup.at[k, at], gup.at[k + 1, at], up_s.at[2 * k + 2 + r],
                    up_r.at[2 * k + 2 + r], s ^ 1, t)

    def down_piece(k, h):
        at = pl.ds(h * cut, cut)
        return copy(w_down.at[halves(s ^ k), at], gdown.at[k, :, at], dn_s.at[2 * k + h],
                    dn_r.at[2 * k + h], s ^ k, t)

    def down_across(k, h):
        at = pl.ds(h * cut, cut)
        return copy(gdown.at[k, :, at], gdown.at[k + 1, :, at], dn_s.at[2 * k + 2 + h],
                    dn_r.at[2 * k + 2 + h], s ^ 1, t)

    def up_send(k):
        for r in range(2):
            up_piece(k, r).start()

    def down_send(k):
        for h in range(cuts):
            down_piece(k, h).start()

    def up_on(k):
        for r in range(2):
            up_piece(k, r).wait_recv()
            up_across(k, r).start()

    def up_arrived(k):
        for r in range(2):
            up_piece(k, r).wait_recv()

    def down_on(k, h):
        down_piece(k, h).wait_recv()
        down_across(k, h).start()

    def downs_on(k):
        for h in range(cuts):
            down_on(k, h)

    def outer_only(fn):
        pl.when(inner == 0)(fn)

    def inner_only(fn):
        pl.when(inner == 1)(fn)

    lat_direct(1).start()
    for k in near:
        lat_direct(k).start()
    every(first_far, lambda k: lat_direct(k).start())
    up_piece(1, 0).start()

    def out_a(k, slot):
        return copy(wo_a, goa.at[slot], oa_s.at[slot], oa_r.at[slot], s, t ^ k)

    def out_b(k, slot):
        return copy(wo_b, gob.at[slot], ob_s.at[slot], ob_r.at[slot], s, t ^ k)

    for k in (2, 1):
        out_a(k, k - 1).start()
        out_b(k, k - 1).start()

    @inner_only
    def _():
        every(last_far, up_send)
        every(first_far, up_send)
        every(first_far, down_send)
        every(last_far, down_send)

    @outer_only
    def _():
        for k in near:
            up_send(k)
        every(first_far, up_send)
        every(last_far, up_send)

    def make_block(k):
        source = lat.at[k]
        at = pl.ds(pl.multiple_of(k * length, length), length)
        wide = source[0:length, :].astype(F32)
        normed = (wide * lax.rsqrt(jnp.mean(wide * wide, axis=-1, keepdims=True) + EPSILON)
                  * lat_gain[...]).astype(BF16)
        rotary = source[length:prow, :].astype(F32).T
        squares = jnp.sum(rotary * rotary, axis=-1, keepdims=True)
        half = ROPE // 2
        turn = table[s ^ k]
        cosine = jnp.concatenate([turn[:, :half], turn[:, :half]], axis=-1)
        sine = jnp.concatenate([-turn[:, half:], turn[:, half:]], axis=-1)

        def turned(w):
            return lax.dot_general(normed, w[...], (((1,), (1,)), ((), ())),
                                   preferred_element_type=F32)

        def keys(flat, gain, nope, heads, dest):
            flat = flat.astype(BF16).astype(F32)
            for h in range(heads):
                piece = flat[:, h * nope:(h + 1) * nope]
                mean = (jnp.sum(piece * piece, axis=-1, keepdims=True) + squares) / (nope + ROPE)
                scale = lax.rsqrt(mean + EPSILON)
                dest[h, at, 0:nope] = (piece * scale * gain[:, 0:nope]).astype(BF16)
                last = rotary * scale * gain[:, nope:nope + ROPE]
                swapped = jnp.concatenate([last[:, half:], last[:, :half]], axis=-1)
                dest[h, at, nope:nope + ROPE] = (
                    last * cosine + swapped * sine).astype(BF16)

        keys(turned(wk_a), gain_a, NOPE_A, heads_a, key_a)
        keys(jnp.dot(normed, wk_b[...], preferred_element_type=F32), gain_b, NOPE_B, heads_b, key_b)
        val_a[at, :] = turned(wv_a).astype(BF16)
        val_b[at, :] = jnp.dot(normed, wv_b[...], preferred_element_type=F32).astype(BF16)

    locals_[2].wait()
    make_block(0)

    def arrived(k):
        lat_direct(k).wait_recv()

    def joined(k):
        copy(lat.at[k, other], lat.at[k, other], latf_s.at[k], latf_r.at[k], s, t ^ 1).wait_recv()
        make_block(k)

    def passed(k):
        arrived(k)
        lat_across(k).start()
        lat_sibling(k).start()

    def relayed(k):
        arrived(k)
        inner_only(lambda: lat_along(k).start())
        lat_across(k).start()
        lat_sibling(k).start()

    def taken(k):
        arrived(k)
        lat_sibling(k).start()

    taken(1)
    for k in near:
        passed(k)
    every(first_far, relayed)
    joined(1)
    every(last_far, relayed)

    @inner_only
    def _():
        for k in near:
            up_send(k)
        for k in near:
            down_send(k)

    up_piece(1, 1).start()
    down_send(1)
    for k in near:
        joined(k)
    for k in near:
        taken(k + 1)
    every(first_far, joined)
    every(first_far + 1, taken)
    every(last_far, joined)
    every(last_far + 1, taken)
    for k in near:
        joined(k + 1)
    every(first_far + 1, joined)
    every(last_far + 1, joined)

    total = n * length
    block = min(total, 2048)
    number = total // block

    def attend(q, key, value, h, depth, width):
        query = q[h * depth:(h + 1) * depth, :].T

        def step(i, state):
            peak, sums, acc = state
            at = pl.ds(pl.multiple_of(i * block, block), block)
            score = lax.dot_general(query, key[h, at, :], (((1,), (1,)), ((), ())),
                                    preferred_element_type=F32) * depth ** (-0.5)
            new = jnp.maximum(peak, jnp.max(score, axis=-1, keepdims=True))
            shifted = jnp.exp(score - new)
            factor = jnp.exp(peak - new)
            sums = sums * factor + jnp.sum(shifted, axis=-1, keepdims=True)
            acc = acc * factor + jnp.dot(
                shifted.astype(BF16), value[at, h * width:(h + 1) * width],
                preferred_element_type=F32)
            return new, sums, acc

        state = (jnp.full((length, 1), -jnp.inf, F32), jnp.zeros((length, 1), F32),
                 jnp.zeros((length, width), F32))
        if number == 1:
            state = step(0, state)
        else:
            state = lax.fori_loop(0, number, step, state)
        return (state[2] / state[1]).astype(BF16)

    for h in range(heads_a):
        res_a = attend(q_a, key_a, val_a, h, depth_a, V_A)
        for j in range(m):
            att[j, :, h * V_A:(h + 1) * V_A] = res_a[j * own:(j + 1) * own]
    for h in range(heads_b):
        res_b = attend(q_b, key_b, val_b, h, depth_b, V_B)
        for j in range(m):
            att[j, :, start_b + h * V_B:start_b + (h + 1) * V_B] = res_b[j * own:(j + 1) * own]

    def row_copy(k):
        return copy(att.at[t ^ k], rows.at[k], at_s.at[k], at_r.at[k], s, t ^ k)

    for k in (2, 3, 1):
        row_copy(k).start()

    def out_on_a():
        return copy(goa.at[1], goa.at[2], oa_s.at[2], oa_r.at[2], s, t ^ 1)

    def out_on_b():
        return copy(gob.at[1], gob.at[2], ob_s.at[2], ob_r.at[2], s, t ^ 1)

    def project(k, slot):
        return (jnp.dot(rows[k, :, 0:width_a], goa[slot], preferred_element_type=F32)
                + jnp.dot(rows[k, :, start_b:], gob[slot], preferred_element_type=F32))

    mixed = (jnp.dot(att[t, :, 0:width_a], wo_a[...], preferred_element_type=F32)
             + jnp.dot(att[t, :, start_b:], wo_b[...], preferred_element_type=F32))
    out_a(1, 0).wait_recv()
    out_b(1, 0).wait_recv()
    row_copy(1).wait_recv()
    mixed += project(1, 0)
    out_a(2, 1).wait_recv()
    out_on_a().start()
    out_b(2, 1).wait_recv()
    out_on_b().start()
    row_copy(2).wait_recv()
    mixed += project(2, 1)
    out_on_a().wait_recv()
    out_on_b().wait_recv()
    row_copy(3).wait_recv()
    mixed += project(3, 2)
    residual = (stream[...].astype(F32) + mixed).astype(BF16)
    res[...] = residual
    wide = residual.astype(F32)
    x[0:own, :] = (wide * lax.rsqrt(jnp.mean(wide * wide, axis=-1, keepdims=True) + EPSILON)
                   * norm_gain[...]).astype(BF16)

    def peer(code):
        return (s ^ 2 if code & 4 else s), t ^ (code & 3)

    bit = own // 2

    class xcopy:
        def __init__(self, src, dst, code):
            self.parts = [
                copy(x.at[pl.ds(src * own + i * bit, bit)], x.at[pl.ds(dst * own + i * bit, bit)],
                     x_s.at[2 * dst + i], x_r.at[2 * dst + i], *peer(code)) for i in range(2)]

        def start(self):
            for c in self.parts:
                c.start()

        def wait_recv(self):
            for c in self.parts:
                c.wait_recv()

        def wait_send(self):
            for c in self.parts:
                c.wait_send()

    def xrelay():
        for i in range(2):
            xcopy(0, 4, 4).parts[i].wait_recv()
            xcopy(4, 6, 2).parts[i].start()
            xcopy(4, 5, 1).parts[i].start()

    xcopy(0, 4, 4).start()
    xcopy(0, 2, 2).start()
    xcopy(0, 1, 1).start()

    @outer_only
    def _():
        for k in near:
            down_send(k)
        every(first_far, lambda k: down_piece(k, 0).start())
        every(last_far, lambda k: down_piece(k, 0).start())
        if cuts > 1:
            every(first_far, lambda k: down_piece(k, 1).start())
            every(last_far, lambda k: down_piece(k, 1).start())

    for k in near:
        up_on(k)
    every(2 * quarter, up_on)
    xcopy(0, 2, 2).wait_recv()
    xcopy(2, 3, 1).start()
    every(3 * quarter, up_on)
    xrelay()

    @outer_only
    def _():
        for k in near:
            downs_on(k)

    xcopy(4, 6, 2).wait_recv()
    xcopy(6, 7, 1).start()

    @inner_only
    def _():
        for k in near:
            downs_on(k)
        every(3 * quarter, downs_on)

    def columns(k, size):
        return pl.ds(pl.multiple_of((s ^ k) * size, 128), size)

    def up(k):
        hid[...] += jnp.dot(x[:, columns(k, wrows)], gup[k], preferred_element_type=F32)

    def up_pair(k):
        up(k)
        up_arrived(k + 1)
        up(k + 1)

    for k in (1, 3, 5, 7):
        xcopy(k - 1, k, 1).wait_recv()
    locals_[3].wait()
    locals_[4].wait()
    hid[...] = jnp.dot(x[:, columns(0, wrows)], gup[0], preferred_element_type=F32)
    up_arrived(1)
    up(1)
    for k in near:
        up_pair(k)
    every(2 * quarter, up_pair)
    every(3 * quarter, up_pair)
    act[...] = jnp.square(jnp.maximum(hid[...], 0.0)).astype(BF16)

    def down(unit, k, h, width):
        base = ((s ^ k) % quarter) * width
        at = pl.ds(pl.multiple_of(base, 128), width)
        first = 0 if h is None else h * cut
        piece = jnp.dot(act[...], gdown[k, :, first:first + width], preferred_element_type=F32)
        for i in range(4):
            even[unit, i, :, at] = piece[2 * i * own:(2 * i + 1) * own]
            odd[unit, i, :, at] = piece[(2 * i + 1) * own:(2 * i + 2) * own].astype(BF16)

    def down_arrived(k):
        for h in range(cuts):
            down_piece(k, h).wait_recv()

    def down_pair(unit):
        def fn(k):
            down(unit, k, None, wcols)
            down_arrived(k + 1)
            down(unit, k + 1, None, wcols)
        return fn

    full = quarter * wcols
    mine_u = zone & 1
    next_u = 1 - mine_u
    places = ((2, s, t ^ 2), (4, s ^ 2, t), (6, s ^ 2, t ^ 2))

    def share(unit, width):
        return copy(odd.at[unit, :, :, 0:width], sib.at[unit, :, :, 0:width],
                    rs_s.at[4 * unit], rs_r.at[4 * unit], s, t ^ 1)

    def deliver(unit, width, i):
        _, sp, tp = places[i]
        return copy(part.at[unit, i, :, 0:width], land.at[unit, i, :, 0:width],
                    rs_s.at[4 * unit + 1 + i], rs_r.at[4 * unit + 1 + i], sp, tp)

    def scatter(unit, width):
        share(unit, width).wait_recv()
        for i in (2, 1, 0):
            part[unit, i, :, 0:width] = (even[unit, i + 1, :, 0:width]
                                         + sib[unit, i + 1, :, 0:width].astype(F32)).astype(BF16)
            deliver(unit, width, i).start()
        even[unit, 0, :, 0:width] += sib[unit, 0, :, 0:width].astype(F32)

    def finish(unit, width, group, h):
        for i in range(3):
            deliver(unit, width, i).wait_recv()
        base = (zone ^ group) * full
        spans = [(0, 0, full)] if h is None or cuts == 1 else [
            (j * cut, j * wcols + h * cut, cut) for j in range(quarter)]
        for lo, to, size in spans:
            at = pl.ds(pl.multiple_of(base + to, 128), size)
            out[:, at] = (res[:, at].astype(F32) + even[unit, 0, :, lo:lo + size]
                          + land[unit, 0, :, lo:lo + size].astype(F32)
                          + land[unit, 1, :, lo:lo + size].astype(F32)
                          + land[unit, 2, :, lo:lo + size].astype(F32)).astype(BF16)

    narrow = quarter * cut

    def far_unit(group, h):
        return 2 + cuts * ((zone ^ group) & 1) + h

    def far(group, h):
        start = group * quarter
        unit = far_unit(group, h)
        every(start, lambda k: down(unit, k, h, cut))
        every(start + 1, lambda k: down_piece(k, h).wait_recv())
        every(start + 1, lambda k: down(unit, k, h, cut))
        share(unit, narrow).start()

    def far_on(h):
        every(2 * quarter, lambda k: down_on(k, h))

    down(mine_u, 0, None, wcols)
    down_arrived(1)
    down(mine_u, 1, None, wcols)
    for k in near:
        if k < quarter:
            down_pair(mine_u)(k)
    share(mine_u, full).start()
    outer_only(lambda: every(3 * quarter, downs_on))
    for k in near:
        if k >= quarter:
            down_pair(next_u)(k)
    share(next_u, full).start()
    scatter(mine_u, full)
    far_on(0)
    for h in range(cuts):
        far(3, h)
        if h == 0:
            scatter(next_u, full)
        else:
            scatter(far_unit(3, h - 1), narrow)
    for h in range(1, cuts):
        far_on(h)
    for h in range(cuts):
        far(2, h)
        if h == 0:
            scatter(far_unit(3, cuts - 1), narrow)
            finish(mine_u, full, 0, None)
            finish(next_u, full, 1, None)
        else:
            scatter(far_unit(2, h - 1), narrow)
    scatter(far_unit(2, cuts - 1), narrow)
    for h in range(cuts):
        finish(far_unit(3, h), narrow, 3, h)
    for h in range(cuts):
        finish(far_unit(2, h), narrow, 2, h)

    lat_direct(1).wait_send()
    up_piece(1, 0).wait_send()
    up_piece(1, 1).wait_send()

    def sent(k):
        lat_across(k).wait_send()
        for r in range(2):
            up_piece(k, r).wait_send()
            up_across(k, r).wait_send()
        for h in range(cuts):
            down_piece(k, h).wait_send()
            down_across(k, h).wait_send()

    for k in near:
        lat_direct(k).wait_send()
        sent(k)
    every(first_far, lambda k: lat_direct(k).wait_send())
    every(first_far, sent)
    every(last_far, sent)

    @inner_only
    def _():
        every(first_far, lambda k: lat_along(k).wait_send())
        every(last_far, lambda k: lat_along(k).wait_send())

    def settled(k, carry):
        lat_sibling(k).wait_send()
        return carry

    lax.fori_loop(1, n, settled, 0)
    for h in range(cuts):
        down_piece(1, h).wait_send()
    for k in (1, 2):
        out_a(k, k - 1).wait_send()
        out_b(k, k - 1).wait_send()
    out_on_a().wait_send()
    out_on_b().wait_send()
    for k in range(1, m):
        row_copy(k).wait_send()
    for src, dst, code in ((0, 4, 4), (0, 2, 2), (0, 1, 1), (2, 3, 1), (4, 6, 2), (4, 5, 1), (6, 7, 1)):
        xcopy(src, dst, code).wait_send()
    units = [(0, full), (1, full)] + [(2 + i, narrow) for i in range(2 * cuts)]
    for unit, width in units:
        share(unit, width).wait_send()
        for i in range(3):
            deliver(unit, width, i).wait_send()


def body(n, m, stream, query_a, query_b, latent, rotary_key, latent_gain, key_gain_a, key_gain_b,
         w_key_a, w_value_a, w_key_b, w_value_b, w_out_a, w_out_b, norm_gain, w_up, w_down):
    length, rank = latent.shape
    own, features = stream.shape
    half = ROPE // 2
    freqs = np.float32(THETA) ** (-np.arange(half, dtype=np.float32) / np.float32(half))
    angle = np.arange(n * length).astype(np.float32)[:, None] * freqs
    cosine, sine = np.cos(angle), np.sin(angle)
    table = jnp.asarray(np.concatenate([cosine, sine], axis=-1).reshape(n, length, ROPE))
    total = n * length
    heads_a = w_key_a.shape[1] // NOPE_A
    heads_b = w_key_b.shape[1] // NOPE_B
    width_a = -(-heads_a * V_A // 128) * 128
    width_b = heads_b * V_B
    hidden = w_up.shape[1] // 2
    V = pltpu.VMEM
    dma = lambda k: pltpu.SemaphoreType.DMA((k,))
    tokens = 2 * m * own
    group = features // 4
    units = 6 if w_down.shape[1] % 256 == 0 else 4
    scratch = [
        V((n, length + ROPE, rank), BF16),
        V((heads_a, total, NOPE_A + ROPE), BF16),
        V((heads_b, total, NOPE_B + ROPE), BF16),
        V((total, heads_a * V_A), BF16),
        V((total, heads_b * V_B), BF16),
        V((m, own, width_a + width_b), BF16),
        V((m, own, width_a + width_b), BF16),
        V((m - 1,) + w_out_a.shape, BF16),
        V((m - 1,) + w_out_b.shape, BF16),
        V((n, w_up.shape[0], hidden), BF16),
        V((n, hidden, w_down.shape[1]), BF16),
        V((tokens, features), BF16),
        V((tokens, hidden), F32),
        V((tokens, hidden), BF16),
        V((own, features), BF16),
        V((units, 4, own, group), F32),
        V((units, 4, own, group), BF16),
        V((units, 4, own, group), BF16),
        V((units, 3, own, group), BF16),
        V((units, 3, own, group), BF16),
        V(table.shape, F32),
    ]
    sizes = [n, n, n, n, n, 3, 3, 3, 3, 2 * n, 2 * n, 2 * n, 2 * n, m, m, 16, 16, 24, 24, 5]
    scratch += [dma(k) for k in sizes]
    vmem = pl.BlockSpec(memory_space=V)
    hbm = pl.BlockSpec(memory_space=pl.ANY)
    return pl.pallas_call(
        functools.partial(kernel, n, m),
        out_shape=jax.ShapeDtypeStruct((own, features), BF16),
        in_specs=[vmem, vmem, vmem, hbm, hbm, hbm, vmem, vmem, vmem, vmem, vmem, vmem, vmem,
                  vmem, vmem, vmem, hbm, hbm],
        out_specs=vmem,
        scratch_shapes=scratch,
        compiler_params=pltpu.CompilerParams(
            collective_id=0, has_side_effects=True, vmem_limit_bytes=67043328),
        name="layer",
    )(stream, query_a.T, query_b.T, latent, rotary_key.T, table, latent_gain[None], key_gain_a[None],
      key_gain_b[None], w_key_a.T, w_value_a.T, w_key_b, w_value_b, w_out_a, w_out_b,
      norm_gain[None], w_up, w_down)


def solution(mesh):
    n, m = mesh.shape["sp"], mesh.shape["tp"]
    in_specs = (
        P(("sp", "tp"), None),
        P("sp", "tp"),
        P("sp", "tp"),
        P("sp", None),
        P("sp", None),
        P(),
        P(),
        P(),
        P(None, "tp"),
        P(None, "tp"),
        P(None, "tp"),
        P(None, "tp"),
        P("tp", None),
        P("tp", None),
        P(),
        P("sp", "tp"),
        P("tp", "sp"),
    )
    out_specs = P(("sp", "tp"), None)
    return jax.shard_map(functools.partial(body, n, m), mesh=mesh, in_specs=in_specs,
                         out_specs=out_specs, check_vma=False)
```

```python
import functools

import jax
import jax.numpy as jnp
import numpy as np
from jax import lax
from jax.experimental import pallas as pl
from jax.experimental.pallas import tpu as pltpu
from jax.sharding import PartitionSpec as P

NOPE_A = 64
V_A = 64
NOPE_B = 128
V_B = 128
ROPE = 32

EPSILON = 1e-06
THETA = 10000.0
F32 = jnp.float32
BF16 = jnp.bfloat16


def kernel(
    n, m,
    stream_h, q_a_h, q_b_h, latent, rotary_t, table_h, lat_gain_h, gain_a_h, gain_b_h,
    wk_a_h, wv_a_h, wk_b_h, wv_b_h, wo_a_h, wo_b_h, norm_gain_h, w_up, w_down,
    out,
    lat, key_a, key_b, val_a, val_b, att, rows, goa, gob,
    gup, gdown, x, hid, act, res, even, odd, sib, part, land, table,
    stream, q_a, q_b, lat_gain, gain_a, gain_b, wk_a, wv_a, wk_b, wv_b, wo_a, wo_b, norm_gain,
    lat_s, lat_r, latf_s, latf_r, oa_s, oa_r, ob_s, ob_r,
    up_s, up_r, dn_s, dn_r, at_s, at_r, x_s, x_r, rs_s, rs_r, loc,
):
    s = lax.axis_index("sp")
    t = lax.axis_index("tp")
    core = t & 1
    length = q_a.shape[1]
    own = stream.shape[0]
    prow = lat.shape[1]
    half_rows = prow // 2
    depth_a = NOPE_A + ROPE
    depth_b = NOPE_B + ROPE
    heads_a = wk_a.shape[0] // NOPE_A
    heads_b = wk_b.shape[1] // NOPE_B
    hidden = gup.shape[2]
    wrows = w_up.shape[0]
    wcols = w_down.shape[1]
    features = stream.shape[1]
    width_a = heads_a * V_A
    width_b = heads_b * V_B
    start_b = att.shape[2] - width_b
    quarter = n // 4
    per = n // 8
    zone = s // quarter
    inner = (zone ^ (zone // 2)) & 1
    near = list(range(2, 2 * quarter, 2))
    first_far = (2 + inner) * quarter
    last_far = (3 - inner) * quarter
    up_half = wrows // 2
    cuts = 2 if wcols % 256 == 0 else 1
    cut = wcols // cuts

    def every(start, fn):
        if per == 1:
            fn(start)
        else:
            def step(j, carry):
                fn(start + 2 * j)
                return carry
            lax.fori_loop(0, per, step, 0)

    def copy(src, dst, ssem, rsem, sp, tp):
        return pltpu.make_async_remote_copy(
            src_ref=src, dst_ref=dst, send_sem=ssem, recv_sem=rsem,
            device_id={"sp": sp, "tp": tp}, device_id_type=pl.DeviceIdType.MESH,
        )

    barrier = pltpu.get_barrier_semaphore()

    def greet(sp, tp):
        pl.semaphore_signal(barrier, inc=1, device_id={"sp": sp, "tp": tp},
                            device_id_type=pl.DeviceIdType.MESH)

    for k in range(1, n):
        greet(s ^ k, t)
    for k in range(1, m):
        greet(s, t ^ k)
    greet(s ^ 2, t ^ 2)

    def halves(target):
        return pl.ds(pl.multiple_of(((target // 2) % 2) * hidden, 128), hidden)

    locals_ = [
        pltpu.make_async_copy(latent, lat.at[0, pl.ds(0, length)], loc.at[0]),
        pltpu.make_async_copy(rotary_t, lat.at[0, pl.ds(length, prow - length)], loc.at[1]),
        pltpu.make_async_copy(table_h, table, loc.at[2]),
        pltpu.make_async_copy(w_up.at[:, halves(s)], gup.at[0], loc.at[3]),
        pltpu.make_async_copy(w_down.at[halves(s)], gdown.at[0], loc.at[4]),
    ]
    early = [pltpu.make_async_copy(a, b, loc.at[5 + i]) for i, (a, b) in enumerate((
        (lat_gain_h, lat_gain), (gain_a_h, gain_a), (gain_b_h, gain_b), (wk_a_h, wk_a),
        (wv_a_h, wv_a), (wk_b_h, wk_b), (wv_b_h, wv_b)))]
    later = [pltpu.make_async_copy(a, b, loc.at[12 + i]) for i, (a, b) in enumerate((
        (q_a_h, q_a), (q_b_h, q_b), (wo_a_h, wo_a), (wo_b_h, wo_b), (stream_h, stream),
        (norm_gain_h, norm_gain)))]
    for c in locals_[:2] + early + locals_[2:] + later:
        c.start()
    locals_[0].wait()
    locals_[1].wait()
    pl.semaphore_wait(barrier, n + m - 1)

    mine = pl.ds(pl.multiple_of(core * half_rows, 16), half_rows)
    other = pl.ds(pl.multiple_of((1 - core) * half_rows, 16), half_rows)

    def lat_direct(k):
        return copy(lat.at[0, mine], lat.at[k, mine], lat_s.at[k], lat_r.at[k], s ^ k, t)

    def lat_across(k):
        return copy(lat.at[k, mine], lat.at[k + 1, mine], lat_s.at[k + 1], lat_r.at[k + 1], s ^ 1, t)

    def lat_sibling(k):
        return copy(lat.at[k, mine], lat.at[k, mine], latf_s.at[k], latf_r.at[k], s, t ^ 1)

    def up_piece(k, r):
        at = pl.ds(r * up_half, up_half)
        return copy(w_up.at[at, halves(s ^ k)], gup.at[k, at], up_s.at[2 * k + r],
                    up_r.at[2 * k + r], s ^ k, t)

    def up_across(k, r):
        at = pl.ds(r * up_half, up_half)
        return copy(gup.at[k, at], gup.at[k + 1, at], up_s.at[2 * k + 2 + r],
                    up_r.at[2 * k + 2 + r], s ^ 1, t)

    def down_piece(k, h):
        at = pl.ds(h * cut, cut)
        return copy(w_down.at[halves(s ^ k), at], gdown.at[k, :, at], dn_s.at[2 * k + h],
                    dn_r.at[2 * k + h], s ^ k, t)

    def down_across(k, h):
        at = pl.ds(h * cut, cut)
        return copy(gdown.at[k, :, at], gdown.at[k + 1, :, at], dn_s.at[2 * k + 2 + h],
                    dn_r.at[2 * k + 2 + h], s ^ 1, t)

    def up_send(k):
        for r in range(2):
            up_piece(k, r).start()

    def down_send(k):
        for h in range(cuts):
            down_piece(k, h).start()

    def up_on(k):
        for r in range(2):
            up_piece(k, r).wait_recv()
            up_across(k, r).start()

    def up_arrived(k):
        for r in range(2):
            up_piece(k, r).wait_recv()

    def down_on(k, h):
        down_piece(k, h).wait_recv()
        down_across(k, h).start()

    def downs_on(k):
        for h in range(cuts):
            down_on(k, h)

    def outer_only(fn):
        pl.when(inner == 0)(fn)

    def inner_only(fn):
        pl.when(inner == 1)(fn)

    lat_direct(1).start()
    for k in near:
        lat_direct(k).start()
    every(first_far, lambda k: lat_direct(k).start())
    every(last_far, lambda k: lat_direct(k).start())
    up_piece(1, 0).start()

    def out_a(k, slot):
        return copy(wo_a_h, goa.at[slot], oa_s.at[slot], oa_r.at[slot], s, t ^ k)

    def out_b(k, slot):
        return copy(wo_b_h, gob.at[slot], ob_s.at[slot], ob_r.at[slot], s, t ^ k)

    for k in (2, 1):
        out_a(k, k - 1).start()
        out_b(k, k - 1).start()

    @inner_only
    def _():
        every(last_far, up_send)
        every(first_far, up_send)
        every(first_far, down_send)
        every(last_far, down_send)
        for k in near:
            up_send(k)

    @outer_only
    def _():
        for k in near:
            up_send(k)
        every(first_far, up_send)
        every(last_far, up_send)

    def make_block(k):
        source = lat.at[k]
        at = pl.ds(pl.multiple_of(k * length, length), length)
        wide = source[0:length, :].astype(F32)
        normed = (wide * lax.rsqrt(jnp.mean(wide * wide, axis=-1, keepdims=True) + EPSILON)
                  * lat_gain[...]).astype(BF16)
        rotary = source[length:prow, :].astype(F32).T
        squares = jnp.sum(rotary * rotary, axis=-1, keepdims=True)
        half = ROPE // 2
        turn = table[s ^ k]
        cosine = jnp.concatenate([turn[:, :half], turn[:, :half]], axis=-1)
        sine = jnp.concatenate([-turn[:, half:], turn[:, half:]], axis=-1)

        def turned(w):
            return lax.dot_general(normed, w[...], (((1,), (1,)), ((), ())),
                                   preferred_element_type=F32)

        def keys(flat, gain, nope, heads, dest):
            flat = flat.astype(BF16).astype(F32)
            for h in range(heads):
                piece = flat[:, h * nope:(h + 1) * nope]
                mean = (jnp.sum(piece * piece, axis=-1, keepdims=True) + squares) / (nope + ROPE)
                scale = lax.rsqrt(mean + EPSILON)
                dest[h, at, 0:nope] = (piece * scale * gain[:, 0:nope]).astype(BF16)
                last = rotary * scale * gain[:, nope:nope + ROPE]
                swapped = jnp.concatenate([last[:, half:], last[:, :half]], axis=-1)
                dest[h, at, nope:nope + ROPE] = (
                    last * cosine + swapped * sine).astype(BF16)

        keys(turned(wk_a), gain_a, NOPE_A, heads_a, key_a)
        keys(jnp.dot(normed, wk_b[...], preferred_element_type=F32), gain_b, NOPE_B, heads_b, key_b)
        val_a[at, :] = turned(wv_a).astype(BF16)
        val_b[at, :] = jnp.dot(normed, wv_b[...], preferred_element_type=F32).astype(BF16)

    locals_[2].wait()
    for c in early:
        c.wait()
    make_block(0)

    def arrived(k):
        lat_direct(k).wait_recv()

    def joined(k):
        copy(lat.at[k, other], lat.at[k, other], latf_s.at[k], latf_r.at[k], s, t ^ 1).wait_recv()
        make_block(k)

    def passed(k):
        arrived(k)
        lat_across(k).start()
        lat_sibling(k).start()

    def taken(k):
        arrived(k)
        lat_sibling(k).start()

    taken(1)
    for k in near:
        passed(k)
    every(first_far, passed)
    joined(1)
    every(last_far, passed)
    up_piece(1, 1).start()
    down_send(1)
    for k in near:
        joined(k)
    for k in near:
        taken(k + 1)
    every(first_far, joined)
    every(first_far + 1, taken)
    every(last_far, joined)
    every(last_far + 1, taken)
    for k in near:
        joined(k + 1)
    every(first_far + 1, joined)
    every(last_far + 1, joined)

    total = n * length
    block = min(total, 2048)
    number = total // block

    def attend(q, key, value, h, depth, width):
        query = q[h * depth:(h + 1) * depth, :].T

        def step(i, state):
            peak, sums, acc = state
            at = pl.ds(pl.multiple_of(i * block, block), block)
            score = lax.dot_general(query, key[h, at, :], (((1,), (1,)), ((), ())),
                                    preferred_element_type=F32) * depth ** (-0.5)
            new = jnp.maximum(peak, jnp.max(score, axis=-1, keepdims=True))
            shifted = jnp.exp(score - new)
            factor = jnp.exp(peak - new)
            sums = sums * factor + jnp.sum(shifted, axis=-1, keepdims=True)
            acc = acc * factor + jnp.dot(
                shifted.astype(BF16), value[at, h * width:(h + 1) * width],
                preferred_element_type=F32)
            return new, sums, acc

        state = (jnp.full((length, 1), -jnp.inf, F32), jnp.zeros((length, 1), F32),
                 jnp.zeros((length, width), F32))
        if number == 1:
            state = step(0, state)
        else:
            state = lax.fori_loop(0, number, step, state)
        return (state[2] / state[1]).astype(BF16)

    for c in later:
        c.wait()
    for h in range(heads_a):
        res_a = attend(q_a, key_a, val_a, h, depth_a, V_A)
        for j in range(m):
            att[j, :, h * V_A:(h + 1) * V_A] = res_a[j * own:(j + 1) * own]
    @inner_only
    def _():
        for k in near:
            up_on(k)

    for h in range(heads_b):
        res_b = attend(q_b, key_b, val_b, h, depth_b, V_B)
        for j in range(m):
            att[j, :, start_b + h * V_B:start_b + (h + 1) * V_B] = res_b[j * own:(j + 1) * own]

    def row_copy(k):
        return copy(att.at[t ^ k], rows.at[k], at_s.at[k], at_r.at[k], s, t ^ k)

    for k in (2, 3, 1):
        row_copy(k).start()

    def out_on_a():
        return copy(goa.at[1], goa.at[2], oa_s.at[2], oa_r.at[2], s, t ^ 1)

    def out_on_b():
        return copy(gob.at[1], gob.at[2], ob_s.at[2], ob_r.at[2], s, t ^ 1)

    def project(k, slot):
        return (jnp.dot(rows[k, :, 0:width_a], goa[slot], preferred_element_type=F32)
                + jnp.dot(rows[k, :, start_b:], gob[slot], preferred_element_type=F32))

    @outer_only
    def _():
        for k in near:
            up_on(k)

    inner_only(lambda: every(2 * quarter, up_on))
    mixed = (jnp.dot(att[t, :, 0:width_a], wo_a[...], preferred_element_type=F32)
             + jnp.dot(att[t, :, start_b:], wo_b[...], preferred_element_type=F32))
    out_a(1, 0).wait_recv()
    out_b(1, 0).wait_recv()
    row_copy(1).wait_recv()
    mixed += project(1, 0)
    out_a(2, 1).wait_recv()
    out_on_a().start()
    out_b(2, 1).wait_recv()
    out_on_b().start()
    row_copy(2).wait_recv()
    mixed += project(2, 1)
    out_on_a().wait_recv()
    out_on_b().wait_recv()
    row_copy(3).wait_recv()
    mixed += project(3, 2)
    residual = (stream[...].astype(F32) + mixed).astype(BF16)
    res[...] = residual
    wide = residual.astype(F32)
    x[0:own, :] = (wide * lax.rsqrt(jnp.mean(wide * wide, axis=-1, keepdims=True) + EPSILON)
                   * norm_gain[...]).astype(BF16)

    def peer(code):
        return (s ^ 2 if code & 4 else s), t ^ (code & 3)

    bit = own // 2

    class xcopy:
        def __init__(self, src, dst, code):
            self.parts = [
                copy(x.at[pl.ds(src * own + i * bit, bit)], x.at[pl.ds(dst * own + i * bit, bit)],
                     x_s.at[2 * dst + i], x_r.at[2 * dst + i], *peer(code)) for i in range(2)]

        def start(self):
            for c in self.parts:
                c.start()

        def wait_recv(self):
            for c in self.parts:
                c.wait_recv()

        def wait_send(self):
            for c in self.parts:
                c.wait_send()

    def xrelay():
        for i in range(2):
            xcopy(0, 4, 4).parts[i].wait_recv()
            xcopy(4, 6, 2).parts[i].start()
            xcopy(4, 5, 1).parts[i].start()

    xcopy(0, 4, 4).start()
    xcopy(0, 2, 2).start()
    xcopy(0, 1, 1).start()

    for k in near:
        down_send(k)

    @outer_only
    def _():
        every(first_far, lambda k: down_piece(k, 0).start())
        every(last_far, lambda k: down_piece(k, 0).start())
        if cuts > 1:
            every(first_far, lambda k: down_piece(k, 1).start())
            every(last_far, lambda k: down_piece(k, 1).start())

    @outer_only
    def _():
        every(3 * quarter, up_on)
        every(2 * quarter, up_on)

    xcopy(0, 2, 2).wait_recv()
    xcopy(2, 3, 1).start()
    xrelay()
    inner_only(lambda: every(3 * quarter, up_on))
    xcopy(4, 6, 2).wait_recv()
    xcopy(6, 7, 1).start()
    for k in near:
        downs_on(k)

    def columns(k, size):
        return pl.ds(pl.multiple_of((s ^ k) * size, 128), size)

    def up(k):
        hid[...] += jnp.dot(x[:, columns(k, wrows)], gup[k], preferred_element_type=F32)

    def up_pair(k):
        up(k)
        up_arrived(k + 1)
        up(k + 1)

    for k in (1, 3, 5, 7):
        xcopy(k - 1, k, 1).wait_recv()
    locals_[3].wait()
    locals_[4].wait()
    hid[...] = jnp.dot(x[:, columns(0, wrows)], gup[0], preferred_element_type=F32)
    up_arrived(1)
    up(1)
    for k in near:
        up_pair(k)
    every(2 * quarter, up_pair)
    every(3 * quarter, up_pair)
    act[...] = jnp.square(jnp.maximum(hid[...], 0.0)).astype(BF16)

    def down(unit, k, h, width):
        base = ((s ^ k) % quarter) * width
        at = pl.ds(pl.multiple_of(base, 128), width)
        first = 0 if h is None else h * cut
        piece = jnp.dot(act[...], gdown[k, :, first:first + width], preferred_element_type=F32)
        for i in range(4):
            even[unit, i, :, at] = piece[2 * i * own:(2 * i + 1) * own]
            odd[unit, i, :, at] = piece[(2 * i + 1) * own:(2 * i + 2) * own].astype(BF16)

    def down_arrived(k):
        for h in range(cuts):
            down_piece(k, h).wait_recv()

    def down_pair(unit):
        def fn(k):
            down(unit, k, None, wcols)
            down_arrived(k + 1)
            down(unit, k + 1, None, wcols)
        return fn

    full = quarter * wcols
    mine_u = zone & 1
    next_u = 1 - mine_u
    places = ((2, s, t ^ 2), (4, s ^ 2, t), (6, s ^ 2, t ^ 2))

    def share(unit, width):
        return copy(odd.at[unit, :, :, 0:width], sib.at[unit, :, :, 0:width],
                    rs_s.at[4 * unit], rs_r.at[4 * unit], s, t ^ 1)

    def deliver(unit, width, i):
        _, sp, tp = places[i]
        return copy(part.at[unit, i, :, 0:width], land.at[unit, i, :, 0:width],
                    rs_s.at[4 * unit + 1 + i], rs_r.at[4 * unit + 1 + i], sp, tp)

    def scatter(unit, width):
        share(unit, width).wait_recv()
        for i in (2, 1, 0):
            part[unit, i, :, 0:width] = (even[unit, i + 1, :, 0:width]
                                         + sib[unit, i + 1, :, 0:width].astype(F32)).astype(BF16)
            deliver(unit, width, i).start()
        even[unit, 0, :, 0:width] += sib[unit, 0, :, 0:width].astype(F32)

    def finish(unit, width, group, h):
        for i in range(3):
            deliver(unit, width, i).wait_recv()
        base = (zone ^ group) * full
        spans = [(0, 0, full)] if h is None or cuts == 1 else [
            (j * cut, j * wcols + h * cut, cut) for j in range(quarter)]
        for lo, to, size in spans:
            at = pl.ds(pl.multiple_of(base + to, 128), size)
            out[:, at] = (res[:, at].astype(F32) + even[unit, 0, :, lo:lo + size]
                          + land[unit, 0, :, lo:lo + size].astype(F32)
                          + land[unit, 1, :, lo:lo + size].astype(F32)
                          + land[unit, 2, :, lo:lo + size].astype(F32)).astype(BF16)

    narrow = quarter * cut

    def far_unit(group, h):
        return 2 + cuts * ((zone ^ group) & 1) + h

    def far(group, h):
        start = group * quarter
        unit = far_unit(group, h)
        every(start, lambda k: down(unit, k, h, cut))
        every(start + 1, lambda k: down_piece(k, h).wait_recv())
        every(start + 1, lambda k: down(unit, k, h, cut))
        share(unit, narrow).start()

    def far_on(group, h):
        every(group * quarter, lambda k: down_on(k, h))

    down(mine_u, 0, None, wcols)
    down_arrived(1)
    down(mine_u, 1, None, wcols)
    for k in near:
        if k < quarter:
            down_pair(mine_u)(k)
    share(mine_u, full).start()
    inner_only(lambda: far_on(2, 0))
    for k in near:
        if k >= quarter:
            down_pair(next_u)(k)
    share(next_u, full).start()
    scatter(mine_u, full)
    for h in range(cuts):
        far_on(3, h)
    outer_only(lambda: far_on(2, 0))
    far(3, 0)
    scatter(next_u, full)
    for h in range(1, cuts):
        far_on(2, h)
        far(3, h)
        scatter(far_unit(3, h - 1), narrow)
    for h in range(cuts):
        far(2, h)
        if h == 0:
            scatter(far_unit(3, cuts - 1), narrow)
        else:
            scatter(far_unit(2, h - 1), narrow)
    finish(mine_u, full, 0, None)
    finish(next_u, full, 1, None)
    scatter(far_unit(2, cuts - 1), narrow)
    for h in range(cuts):
        finish(far_unit(3, h), narrow, 3, h)
    for h in range(cuts):
        finish(far_unit(2, h), narrow, 2, h)

    lat_direct(1).wait_send()
    up_piece(1, 0).wait_send()
    up_piece(1, 1).wait_send()

    def sent(k):
        lat_across(k).wait_send()
        for r in range(2):
            up_piece(k, r).wait_send()
            up_across(k, r).wait_send()
        for h in range(cuts):
            down_piece(k, h).wait_send()
            down_across(k, h).wait_send()

    for k in near:
        lat_direct(k).wait_send()
        sent(k)
    every(first_far, lambda k: lat_direct(k).wait_send())
    every(last_far, lambda k: lat_direct(k).wait_send())
    every(first_far, sent)
    every(last_far, sent)

    def settled(k, carry):
        lat_sibling(k).wait_send()
        return carry

    lax.fori_loop(1, n, settled, 0)
    for h in range(cuts):
        down_piece(1, h).wait_send()
    for k in (1, 2):
        out_a(k, k - 1).wait_send()
        out_b(k, k - 1).wait_send()
    out_on_a().wait_send()
    out_on_b().wait_send()
    for k in range(1, m):
        row_copy(k).wait_send()
    for src, dst, code in ((0, 4, 4), (0, 2, 2), (0, 1, 1), (2, 3, 1), (4, 6, 2), (4, 5, 1), (6, 7, 1)):
        xcopy(src, dst, code).wait_send()
    units = [(0, full), (1, full)] + [(2 + i, narrow) for i in range(2 * cuts)]
    for unit, width in units:
        share(unit, width).wait_send()
        for i in range(3):
            deliver(unit, width, i).wait_send()


def body(n, m, stream, query_a, query_b, latent, rotary_key, latent_gain, key_gain_a, key_gain_b,
         w_key_a, w_value_a, w_key_b, w_value_b, w_out_a, w_out_b, norm_gain, w_up, w_down):
    length, rank = latent.shape
    own, features = stream.shape
    half = ROPE // 2
    freqs = np.float32(THETA) ** (-np.arange(half, dtype=np.float32) / np.float32(half))
    angle = np.arange(n * length).astype(np.float32)[:, None] * freqs
    cosine, sine = np.cos(angle), np.sin(angle)
    table = jnp.asarray(np.concatenate([cosine, sine], axis=-1).reshape(n, length, ROPE))
    total = n * length
    heads_a = w_key_a.shape[1] // NOPE_A
    heads_b = w_key_b.shape[1] // NOPE_B
    width_a = -(-heads_a * V_A // 128) * 128
    width_b = heads_b * V_B
    hidden = w_up.shape[1] // 2
    V = pltpu.VMEM
    dma = lambda k: pltpu.SemaphoreType.DMA((k,))
    tokens = 2 * m * own
    group = features // 4
    units = 6 if w_down.shape[1] % 256 == 0 else 4
    scratch = [
        V((n, length + ROPE, rank), BF16),
        V((heads_a, total, NOPE_A + ROPE), BF16),
        V((heads_b, total, NOPE_B + ROPE), BF16),
        V((total, heads_a * V_A), BF16),
        V((total, heads_b * V_B), BF16),
        V((m, own, width_a + width_b), BF16),
        V((m, own, width_a + width_b), BF16),
        V((m - 1,) + w_out_a.shape, BF16),
        V((m - 1,) + w_out_b.shape, BF16),
        V((n, w_up.shape[0], hidden), BF16),
        V((n, hidden, w_down.shape[1]), BF16),
        V((tokens, features), BF16),
        V((tokens, hidden), F32),
        V((tokens, hidden), BF16),
        V((own, features), BF16),
        V((units, 4, own, group), F32),
        V((units, 4, own, group), BF16),
        V((units, 4, own, group), BF16),
        V((units, 3, own, group), BF16),
        V((units, 3, own, group), BF16),
        V(table.shape, F32),
    ]
    given = (stream, query_a.T, query_b.T, latent_gain[None], key_gain_a[None], key_gain_b[None],
             w_key_a.T, w_value_a.T, w_key_b, w_value_b, w_out_a, w_out_b, norm_gain[None])
    scratch += [V(a.shape, a.dtype) for a in given]
    sizes = [n, n, n, n, 3, 3, 3, 3, 2 * n, 2 * n, 2 * n, 2 * n, m, m, 16, 16, 24, 24, 18]
    scratch += [dma(k) for k in sizes]
    vmem = pl.BlockSpec(memory_space=V)
    hbm = pl.BlockSpec(memory_space=pl.ANY)
    return pl.pallas_call(
        functools.partial(kernel, n, m),
        out_shape=jax.ShapeDtypeStruct((own, features), BF16),
        in_specs=[hbm] * 18,
        out_specs=vmem,
        scratch_shapes=scratch,
        compiler_params=pltpu.CompilerParams(
            collective_id=0, has_side_effects=True, vmem_limit_bytes=67043328),
        name="layer",
    )(stream, query_a.T, query_b.T, latent, rotary_key.T, table, latent_gain[None], key_gain_a[None],
      key_gain_b[None], w_key_a.T, w_value_a.T, w_key_b, w_value_b, w_out_a, w_out_b,
      norm_gain[None], w_up, w_down)


def solution(mesh):
    n, m = mesh.shape["sp"], mesh.shape["tp"]
    in_specs = (
        P(("sp", "tp"), None),
        P("sp", "tp"),
        P("sp", "tp"),
        P("sp", None),
        P("sp", None),
        P(),
        P(),
        P(),
        P(None, "tp"),
        P(None, "tp"),
        P(None, "tp"),
        P(None, "tp"),
        P("tp", None),
        P("tp", None),
        P(),
        P("sp", "tp"),
        P("tp", "sp"),
    )
    out_specs = P(("sp", "tp"), None)
    return jax.shard_map(functools.partial(body, n, m), mesh=mesh, in_specs=in_specs,
                         out_specs=out_specs, check_vma=False)
```

```python
import functools

import jax
import jax.numpy as jnp
import numpy as np
from jax import lax
from jax.experimental import pallas as pl
from jax.experimental.pallas import tpu as pltpu
from jax.sharding import PartitionSpec as P

NOPE_A = 64
V_A = 64
NOPE_B = 128
V_B = 128
ROPE = 32

EPSILON = 1e-06
THETA = 10000.0
F32 = jnp.float32
BF16 = jnp.bfloat16


def kernel(
    n, m,
    stream_h, q_a_h, q_b_h, latent, rotary_t, table_h, lat_gain_h, gain_a_h, gain_b_h,
    wk_a_h, wv_a_h, wk_b_h, wv_b_h, wo_a_h, wo_b_h, norm_gain_h, w_up, w_down,
    out,
    lat, key_a, key_b, val_a, val_b, att, rows, goa, gob,
    gup, gdown, x, hid, act, res, even, odd, sib, part, land, table,
    stream, q_a, q_b, lat_gain, gain_a, gain_b, wk_a, wv_a, wk_b, wv_b, wo_a, wo_b, norm_gain,
    lat_s, lat_r, latf_s, latf_r, oa_s, oa_r, ob_s, ob_r,
    up_s, up_r, dn_s, dn_r, at_s, at_r, x_s, x_r, rs_s, rs_r, loc,
):
    s = lax.axis_index("sp")
    t = lax.axis_index("tp")
    core = t & 1
    length = q_a.shape[1]
    own = stream.shape[0]
    prow = lat.shape[1]
    half_rows = prow // 2
    depth_a = NOPE_A + ROPE
    depth_b = NOPE_B + ROPE
    heads_a = wk_a.shape[0] // NOPE_A
    heads_b = wk_b.shape[1] // NOPE_B
    hidden = gup.shape[2]
    wrows = w_up.shape[0]
    wcols = w_down.shape[1]
    features = stream.shape[1]
    width_a = heads_a * V_A
    width_b = heads_b * V_B
    start_b = att.shape[2] - width_b
    quarter = n // 4
    per = n // 8
    zone = s // quarter
    inner = (zone ^ (zone // 2)) & 1
    near = list(range(2, 2 * quarter, 2))
    first_far = (2 + inner) * quarter
    last_far = (3 - inner) * quarter
    up_half = wrows // 2
    cuts = 2 if wcols % 256 == 0 else 1
    cut = wcols // cuts

    def every(start, fn):
        if per == 1:
            fn(start)
        else:
            def step(j, carry):
                fn(start + 2 * j)
                return carry
            lax.fori_loop(0, per, step, 0)

    def copy(src, dst, ssem, rsem, sp, tp):
        return pltpu.make_async_remote_copy(
            src_ref=src, dst_ref=dst, send_sem=ssem, recv_sem=rsem,
            device_id={"sp": sp, "tp": tp}, device_id_type=pl.DeviceIdType.MESH,
        )

    barrier = pltpu.get_barrier_semaphore()

    def greet(sp, tp):
        pl.semaphore_signal(barrier, inc=1, device_id={"sp": sp, "tp": tp},
                            device_id_type=pl.DeviceIdType.MESH)

    for k in range(1, n):
        greet(s ^ k, t)
    for k in range(1, m):
        greet(s, t ^ k)
    greet(s ^ 2, t ^ 2)

    def halves(target):
        return pl.ds(pl.multiple_of(((target // 2) % 2) * hidden, 128), hidden)

    locals_ = [
        pltpu.make_async_copy(latent, lat.at[0, pl.ds(0, length)], loc.at[0]),
        pltpu.make_async_copy(rotary_t, lat.at[0, pl.ds(length, prow - length)], loc.at[1]),
        pltpu.make_async_copy(table_h, table, loc.at[2]),
        pltpu.make_async_copy(w_up.at[:, halves(s)], gup.at[0], loc.at[3]),
        pltpu.make_async_copy(w_down.at[halves(s)], gdown.at[0], loc.at[4]),
    ]
    early = [pltpu.make_async_copy(a, b, loc.at[5 + i]) for i, (a, b) in enumerate((
        (lat_gain_h, lat_gain), (gain_a_h, gain_a), (gain_b_h, gain_b), (wk_a_h, wk_a),
        (wv_a_h, wv_a), (wk_b_h, wk_b), (wv_b_h, wv_b)))]
    later = [pltpu.make_async_copy(a, b, loc.at[12 + i]) for i, (a, b) in enumerate((
        (q_a_h, q_a), (q_b_h, q_b), (wo_a_h, wo_a), (wo_b_h, wo_b), (stream_h, stream),
        (norm_gain_h, norm_gain)))]
    for c in locals_[:2] + early + locals_[2:] + later:
        c.start()
    locals_[0].wait()
    locals_[1].wait()
    pl.semaphore_wait(barrier, n + m - 1)

    mine = pl.ds(pl.multiple_of(core * half_rows, 16), half_rows)
    other = pl.ds(pl.multiple_of((1 - core) * half_rows, 16), half_rows)

    def lat_direct(k):
        return copy(lat.at[0, mine], lat.at[k, mine], lat_s.at[0], lat_r.at[k], s ^ k, t)

    def lat_across(k):
        return copy(lat.at[k, mine], lat.at[k + 1, mine], lat_s.at[0], lat_r.at[k + 1], s ^ 1, t)

    def lat_sibling(k):
        return copy(lat.at[k, mine], lat.at[k, mine], latf_s.at[0], latf_r.at[k], s, t ^ 1)

    def up_piece(k, r):
        at = pl.ds(r * up_half, up_half)
        return copy(w_up.at[at, halves(s ^ k)], gup.at[k, at], up_s.at[0],
                    up_r.at[2 * k + r], s ^ k, t)

    def up_across(k, r):
        at = pl.ds(r * up_half, up_half)
        return copy(gup.at[k, at], gup.at[k + 1, at], up_s.at[0],
                    up_r.at[2 * k + 2 + r], s ^ 1, t)

    def down_piece(k, h):
        at = pl.ds(h * cut, cut)
        return copy(w_down.at[halves(s ^ k), at], gdown.at[k, :, at], dn_s.at[0],
                    dn_r.at[2 * k + h], s ^ k, t)

    def down_across(k, h):
        at = pl.ds(h * cut, cut)
        return copy(gdown.at[k, :, at], gdown.at[k + 1, :, at], dn_s.at[0],
                    dn_r.at[2 * k + 2 + h], s ^ 1, t)

    def up_send(k):
        for r in range(2):
            up_piece(k, r).start()

    def down_send(k):
        for h in range(cuts):
            down_piece(k, h).start()

    def up_on(k):
        for r in range(2):
            up_piece(k, r).wait_recv()
            up_across(k, r).start()

    def up_arrived(k):
        for r in range(2):
            up_piece(k, r).wait_recv()

    def down_on(k, h):
        down_piece(k, h).wait_recv()
        down_across(k, h).start()

    def downs_on(k):
        for h in range(cuts):
            down_on(k, h)

    def outer_only(fn):
        pl.when(inner == 0)(fn)

    def inner_only(fn):
        pl.when(inner == 1)(fn)

    lat_direct(1).start()
    for k in near:
        lat_direct(k).start()
    every(first_far, lambda k: lat_direct(k).start())
    every(last_far, lambda k: lat_direct(k).start())
    up_piece(1, 0).start()

    def out_a(k, slot):
        return copy(wo_a_h, goa.at[slot], oa_s.at[0], oa_r.at[slot], s, t ^ k)

    def out_b(k, slot):
        return copy(wo_b_h, gob.at[slot], ob_s.at[0], ob_r.at[slot], s, t ^ k)

    for k in (2, 1):
        out_a(k, k - 1).start()
        out_b(k, k - 1).start()

    @inner_only
    def _():
        every(last_far, up_send)
        every(first_far, up_send)
        every(first_far, down_send)
        every(last_far, down_send)
        for k in near:
            up_send(k)

    @outer_only
    def _():
        for k in near:
            up_send(k)
        every(first_far, up_send)
        every(last_far, up_send)

    def make_block(k):
        source = lat.at[k]
        at = pl.ds(pl.multiple_of(k * length, length), length)
        wide = source[0:length, :].astype(F32)
        normed = (wide * lax.rsqrt(jnp.mean(wide * wide, axis=-1, keepdims=True) + EPSILON)
                  * lat_gain[...]).astype(BF16)
        rotary = source[length:prow, :].astype(F32).T
        squares = jnp.sum(rotary * rotary, axis=-1, keepdims=True)
        half = ROPE // 2
        turn = table[s ^ k]
        cosine = jnp.concatenate([turn[:, :half], turn[:, :half]], axis=-1)
        sine = jnp.concatenate([-turn[:, half:], turn[:, half:]], axis=-1)

        def turned(w):
            return lax.dot_general(normed, w[...], (((1,), (1,)), ((), ())),
                                   preferred_element_type=F32)

        def keys(flat, gain, nope, heads, dest):
            flat = flat.astype(BF16).astype(F32)
            for h in range(heads):
                piece = flat[:, h * nope:(h + 1) * nope]
                mean = (jnp.sum(piece * piece, axis=-1, keepdims=True) + squares) / (nope + ROPE)
                scale = lax.rsqrt(mean + EPSILON)
                dest[h, at, 0:nope] = (piece * scale * gain[:, 0:nope]).astype(BF16)
                last = rotary * scale * gain[:, nope:nope + ROPE]
                swapped = jnp.concatenate([last[:, half:], last[:, :half]], axis=-1)
                dest[h, at, nope:nope + ROPE] = (
                    last * cosine + swapped * sine).astype(BF16)

        keys(turned(wk_a), gain_a, NOPE_A, heads_a, key_a)
        keys(jnp.dot(normed, wk_b[...], preferred_element_type=F32), gain_b, NOPE_B, heads_b, key_b)
        val_a[at, :] = turned(wv_a).astype(BF16)
        val_b[at, :] = jnp.dot(normed, wv_b[...], preferred_element_type=F32).astype(BF16)

    locals_[2].wait()
    for c in early:
        c.wait()
    make_block(0)

    def arrived(k):
        lat_direct(k).wait_recv()

    def joined(k):
        copy(lat.at[k, other], lat.at[k, other], latf_s.at[0], latf_r.at[k], s, t ^ 1).wait_recv()
        make_block(k)

    def passed(k):
        arrived(k)
        lat_across(k).start()
        lat_sibling(k).start()

    def taken(k):
        arrived(k)
        lat_sibling(k).start()

    taken(1)
    for k in near:
        passed(k)
    every(first_far, passed)
    joined(1)
    every(last_far, passed)
    up_piece(1, 1).start()
    down_send(1)
    for k in near:
        joined(k)
    for k in near:
        taken(k + 1)
    every(first_far, joined)
    every(first_far + 1, taken)
    every(last_far, joined)
    every(last_far + 1, taken)
    for k in near:
        joined(k + 1)
    every(first_far + 1, joined)
    every(last_far + 1, joined)

    total = n * length
    block = min(total, 2048)
    number = total // block

    def attend(q, key, value, h, depth, width):
        query = q[h * depth:(h + 1) * depth, :].T

        def step(i, state):
            peak, sums, acc = state
            at = pl.ds(pl.multiple_of(i * block, block), block)
            score = lax.dot_general(query, key[h, at, :], (((1,), (1,)), ((), ())),
                                    preferred_element_type=F32) * depth ** (-0.5)
            new = jnp.maximum(peak, jnp.max(score, axis=-1, keepdims=True))
            shifted = jnp.exp(score - new)
            factor = jnp.exp(peak - new)
            sums = sums * factor + jnp.sum(shifted, axis=-1, keepdims=True)
            acc = acc * factor + jnp.dot(
                shifted.astype(BF16), value[at, h * width:(h + 1) * width],
                preferred_element_type=F32)
            return new, sums, acc

        state = (jnp.full((length, 1), -jnp.inf, F32), jnp.zeros((length, 1), F32),
                 jnp.zeros((length, width), F32))
        if number == 1:
            state = step(0, state)
        else:
            state = lax.fori_loop(0, number, step, state)
        return (state[2] / state[1]).astype(BF16)

    for c in later:
        c.wait()
    for h in range(heads_a):
        res_a = attend(q_a, key_a, val_a, h, depth_a, V_A)
        for j in range(m):
            att[j, :, h * V_A:(h + 1) * V_A] = res_a[j * own:(j + 1) * own]
    @inner_only
    def _():
        for k in near:
            up_on(k)

    for h in range(heads_b):
        res_b = attend(q_b, key_b, val_b, h, depth_b, V_B)
        for j in range(m):
            att[j, :, start_b + h * V_B:start_b + (h + 1) * V_B] = res_b[j * own:(j + 1) * own]

    def row_copy(k):
        return copy(att.at[t ^ k], rows.at[k], at_s.at[0], at_r.at[k], s, t ^ k)

    for k in (2, 3, 1):
        row_copy(k).start()

    def out_on_a():
        return copy(goa.at[1], goa.at[2], oa_s.at[0], oa_r.at[2], s, t ^ 1)

    def out_on_b():
        return copy(gob.at[1], gob.at[2], ob_s.at[0], ob_r.at[2], s, t ^ 1)

    def project(k, slot):
        return (jnp.dot(rows[k, :, 0:width_a], goa[slot], preferred_element_type=F32)
                + jnp.dot(rows[k, :, start_b:], gob[slot], preferred_element_type=F32))

    @outer_only
    def _():
        for k in near:
            up_on(k)

    inner_only(lambda: every(2 * quarter, up_on))
    mixed = (jnp.dot(att[t, :, 0:width_a], wo_a[...], preferred_element_type=F32)
             + jnp.dot(att[t, :, start_b:], wo_b[...], preferred_element_type=F32))
    out_a(1, 0).wait_recv()
    out_b(1, 0).wait_recv()
    row_copy(1).wait_recv()
    mixed += project(1, 0)
    out_a(2, 1).wait_recv()
    out_on_a().start()
    out_b(2, 1).wait_recv()
    out_on_b().start()
    row_copy(2).wait_recv()
    mixed += project(2, 1)
    out_on_a().wait_recv()
    out_on_b().wait_recv()
    row_copy(3).wait_recv()
    mixed += project(3, 2)
    residual = (stream[...].astype(F32) + mixed).astype(BF16)
    res[...] = residual
    wide = residual.astype(F32)
    x[0:own, :] = (wide * lax.rsqrt(jnp.mean(wide * wide, axis=-1, keepdims=True) + EPSILON)
                   * norm_gain[...]).astype(BF16)

    def peer(code):
        return (s ^ 2 if code & 4 else s), t ^ (code & 3)

    bit = own // 2

    class xcopy:
        def __init__(self, src, dst, code):
            self.parts = [
                copy(x.at[pl.ds(src * own + i * bit, bit)], x.at[pl.ds(dst * own + i * bit, bit)],
                     x_s.at[0], x_r.at[2 * dst + i], *peer(code)) for i in range(2)]

        def start(self):
            for c in self.parts:
                c.start()

        def wait_recv(self):
            for c in self.parts:
                c.wait_recv()

        def wait_send(self):
            for c in self.parts:
                c.wait_send()

    def xrelay():
        for i in range(2):
            xcopy(0, 4, 4).parts[i].wait_recv()
            xcopy(4, 6, 2).parts[i].start()
            xcopy(4, 5, 1).parts[i].start()

    xcopy(0, 4, 4).start()
    xcopy(0, 2, 2).start()
    xcopy(0, 1, 1).start()

    for k in near:
        down_send(k)

    @outer_only
    def _():
        every(first_far, lambda k: down_piece(k, 0).start())
        every(last_far, lambda k: down_piece(k, 0).start())
        if cuts > 1:
            every(first_far, lambda k: down_piece(k, 1).start())
            every(last_far, lambda k: down_piece(k, 1).start())

    @outer_only
    def _():
        every(3 * quarter, up_on)
        every(2 * quarter, up_on)

    xcopy(0, 2, 2).wait_recv()
    xcopy(2, 3, 1).start()
    xrelay()
    inner_only(lambda: every(3 * quarter, up_on))
    xcopy(4, 6, 2).wait_recv()
    xcopy(6, 7, 1).start()
    for k in near:
        downs_on(k)

    def columns(k, size):
        return pl.ds(pl.multiple_of((s ^ k) * size, 128), size)

    def up(k):
        hid[...] += jnp.dot(x[:, columns(k, wrows)], gup[k], preferred_element_type=F32)

    def up_pair(k):
        up(k)
        up_arrived(k + 1)
        up(k + 1)

    for k in (1, 3, 5, 7):
        xcopy(k - 1, k, 1).wait_recv()
    locals_[3].wait()
    locals_[4].wait()
    hid[...] = jnp.dot(x[:, columns(0, wrows)], gup[0], preferred_element_type=F32)
    up_arrived(1)
    up(1)
    for k in near:
        up_pair(k)
    every(2 * quarter, up_pair)
    every(3 * quarter, up_pair)
    act[...] = jnp.square(jnp.maximum(hid[...], 0.0)).astype(BF16)

    def down(unit, k, h, width):
        base = ((s ^ k) % quarter) * width
        at = pl.ds(pl.multiple_of(base, 128), width)
        first = 0 if h is None else h * cut
        piece = jnp.dot(act[...], gdown[k, :, first:first + width], preferred_element_type=F32)
        for i in range(4):
            even[unit, i, :, at] = piece[2 * i * own:(2 * i + 1) * own]
            odd[unit, i, :, at] = piece[(2 * i + 1) * own:(2 * i + 2) * own].astype(BF16)

    def down_arrived(k):
        for h in range(cuts):
            down_piece(k, h).wait_recv()

    def down_pair(unit):
        def fn(k):
            down(unit, k, None, wcols)
            down_arrived(k + 1)
            down(unit, k + 1, None, wcols)
        return fn

    full = quarter * wcols
    mine_u = zone & 1
    next_u = 1 - mine_u
    places = ((2, s, t ^ 2), (4, s ^ 2, t), (6, s ^ 2, t ^ 2))

    def share(unit, width):
        return copy(odd.at[unit, :, :, 0:width], sib.at[unit, :, :, 0:width],
                    rs_s.at[0], rs_r.at[4 * unit], s, t ^ 1)

    def deliver(unit, width, i):
        _, sp, tp = places[i]
        return copy(part.at[unit, i, :, 0:width], land.at[unit, i, :, 0:width],
                    rs_s.at[0], rs_r.at[4 * unit + 1 + i], sp, tp)

    def scatter(unit, width):
        share(unit, width).wait_recv()
        for i in (2, 1, 0):
            part[unit, i, :, 0:width] = (even[unit, i + 1, :, 0:width]
                                         + sib[unit, i + 1, :, 0:width].astype(F32)).astype(BF16)
            deliver(unit, width, i).start()
        even[unit, 0, :, 0:width] += sib[unit, 0, :, 0:width].astype(F32)

    def finish(unit, width, group, h):
        for i in range(3):
            deliver(unit, width, i).wait_recv()
        base = (zone ^ group) * full
        spans = [(0, 0, full)] if h is None or cuts == 1 else [
            (j * cut, j * wcols + h * cut, cut) for j in range(quarter)]
        for lo, to, size in spans:
            at = pl.ds(pl.multiple_of(base + to, 128), size)
            out[:, at] = (res[:, at].astype(F32) + even[unit, 0, :, lo:lo + size]
                          + land[unit, 0, :, lo:lo + size].astype(F32)
                          + land[unit, 1, :, lo:lo + size].astype(F32)
                          + land[unit, 2, :, lo:lo + size].astype(F32)).astype(BF16)

    narrow = quarter * cut

    def far_unit(group, h):
        return 2 + cuts * ((zone ^ group) & 1) + h

    def far(group, h):
        start = group * quarter
        unit = far_unit(group, h)
        every(start, lambda k: down(unit, k, h, cut))
        every(start + 1, lambda k: down_piece(k, h).wait_recv())
        every(start + 1, lambda k: down(unit, k, h, cut))
        share(unit, narrow).start()

    def far_on(group, h):
        every(group * quarter, lambda k: down_on(k, h))

    down(mine_u, 0, None, wcols)
    down_arrived(1)
    down(mine_u, 1, None, wcols)
    for k in near:
        if k < quarter:
            down_pair(mine_u)(k)
    share(mine_u, full).start()
    inner_only(lambda: far_on(2, 0))
    for k in near:
        if k >= quarter:
            down_pair(next_u)(k)
    share(next_u, full).start()
    scatter(mine_u, full)
    for h in range(cuts):
        far_on(3, h)
    outer_only(lambda: far_on(2, 0))
    far(3, 0)
    scatter(next_u, full)
    for h in range(1, cuts):
        far_on(2, h)
        far(3, h)
        scatter(far_unit(3, h - 1), narrow)
    for h in range(cuts):
        far(2, h)
        if h == 0:
            scatter(far_unit(3, cuts - 1), narrow)
        else:
            scatter(far_unit(2, h - 1), narrow)
    finish(mine_u, full, 0, None)
    finish(next_u, full, 1, None)
    scatter(far_unit(2, cuts - 1), narrow)
    for h in range(cuts):
        finish(far_unit(3, h), narrow, 3, h)
    for h in range(cuts):
        finish(far_unit(2, h), narrow, 2, h)

    def drained(ref, sem):
        copy(ref, ref, sem.at[0], sem.at[0], s, t ^ 1).wait_send()

    drained(lat.at[pl.ds(1, n - 1), mine], lat_s)
    drained(lat.at[pl.ds(1, n - 1), mine], latf_s)
    drained(gup.at[pl.ds(1, n - 1)], up_s)
    drained(gdown.at[pl.ds(1, n - 1)], dn_s)
    drained(goa, oa_s)
    drained(gob, ob_s)
    drained(rows.at[pl.ds(1, m - 1)], at_s)
    drained(x.at[pl.ds(own, 7 * own)], x_s)
    drained(x.at[pl.ds(0, 7 * own)], rs_s)


def body(n, m, stream, query_a, query_b, latent, rotary_key, latent_gain, key_gain_a, key_gain_b,
         w_key_a, w_value_a, w_key_b, w_value_b, w_out_a, w_out_b, norm_gain, w_up, w_down):
    length, rank = latent.shape
    own, features = stream.shape
    half = ROPE // 2
    freqs = np.float32(THETA) ** (-np.arange(half, dtype=np.float32) / np.float32(half))
    angle = np.arange(n * length).astype(np.float32)[:, None] * freqs
    cosine, sine = np.cos(angle), np.sin(angle)
    table = jnp.asarray(np.concatenate([cosine, sine], axis=-1).reshape(n, length, ROPE))
    total = n * length
    heads_a = w_key_a.shape[1] // NOPE_A
    heads_b = w_key_b.shape[1] // NOPE_B
    width_a = -(-heads_a * V_A // 128) * 128
    width_b = heads_b * V_B
    hidden = w_up.shape[1] // 2
    V = pltpu.VMEM
    dma = lambda k: pltpu.SemaphoreType.DMA((k,))
    tokens = 2 * m * own
    group = features // 4
    units = 6 if w_down.shape[1] % 256 == 0 else 4
    scratch = [
        V((n, length + ROPE, rank), BF16),
        V((heads_a, total, NOPE_A + ROPE), BF16),
        V((heads_b, total, NOPE_B + ROPE), BF16),
        V((total, heads_a * V_A), BF16),
        V((total, heads_b * V_B), BF16),
        V((m, own, width_a + width_b), BF16),
        V((m, own, width_a + width_b), BF16),
        V((m - 1,) + w_out_a.shape, BF16),
        V((m - 1,) + w_out_b.shape, BF16),
        V((n, w_up.shape[0], hidden), BF16),
        V((n, hidden, w_down.shape[1]), BF16),
        V((tokens, features), BF16),
        V((tokens, hidden), F32),
        V((tokens, hidden), BF16),
        V((own, features), BF16),
        V((units, 4, own, group), F32),
        V((units, 4, own, group), BF16),
        V((units, 4, own, group), BF16),
        V((units, 3, own, group), BF16),
        V((units, 3, own, group), BF16),
        V(table.shape, F32),
    ]
    given = (stream, query_a.T, query_b.T, latent_gain[None], key_gain_a[None], key_gain_b[None],
             w_key_a.T, w_value_a.T, w_key_b, w_value_b, w_out_a, w_out_b, norm_gain[None])
    scratch += [V(a.shape, a.dtype) for a in given]
    sizes = [1, n, 1, n, 1, 3, 1, 3, 1, 2 * n, 1, 2 * n, 1, m, 1, 16, 1, 24, 18]
    scratch += [dma(k) for k in sizes]
    vmem = pl.BlockSpec(memory_space=V)
    hbm = pl.BlockSpec(memory_space=pl.ANY)
    return pl.pallas_call(
        functools.partial(kernel, n, m),
        out_shape=jax.ShapeDtypeStruct((own, features), BF16),
        in_specs=[hbm] * 18,
        out_specs=vmem,
        scratch_shapes=scratch,
        compiler_params=pltpu.CompilerParams(
            collective_id=0, has_side_effects=True, vmem_limit_bytes=67043328),
        name="layer",
    )(stream, query_a.T, query_b.T, latent, rotary_key.T, table, latent_gain[None], key_gain_a[None],
      key_gain_b[None], w_key_a.T, w_value_a.T, w_key_b, w_value_b, w_out_a, w_out_b,
      norm_gain[None], w_up, w_down)


def solution(mesh):
    n, m = mesh.shape["sp"], mesh.shape["tp"]
    in_specs = (
        P(("sp", "tp"), None),
        P("sp", "tp"),
        P("sp", "tp"),
        P("sp", None),
        P("sp", None),
        P(),
        P(),
        P(),
        P(None, "tp"),
        P(None, "tp"),
        P(None, "tp"),
        P(None, "tp"),
        P("tp", None),
        P("tp", None),
        P(),
        P("sp", "tp"),
        P("tp", "sp"),
    )
    out_specs = P(("sp", "tp"), None)
    return jax.shard_map(functools.partial(body, n, m), mesh=mesh, in_specs=in_specs,
                         out_specs=out_specs, check_vma=False)
```

```python
import functools

import jax
import jax.numpy as jnp
import numpy as np
from jax import lax
from jax.experimental import pallas as pl
from jax.experimental.pallas import tpu as pltpu
from jax.sharding import PartitionSpec as P

NOPE_A = 64
V_A = 64
NOPE_B = 128
V_B = 128
ROPE = 32

EPSILON = 1e-06
THETA = 10000.0
F32 = jnp.float32
BF16 = jnp.bfloat16


class Several:
    def __init__(self, parts):
        self.parts = parts

    def start(self):
        for c in self.parts:
            c.start()

    def wait_recv(self):
        for c in self.parts:
            c.wait_recv()


def kernel(
    n, m,
    stream_h, q_a_h, q_b_h, latent, rotary_t, table_h, lat_gain_h, gain_a_h, gain_b_h,
    wk_a_h, wv_a_h, wk_b_h, wv_b_h, wo_a_h, wo_b_h, norm_gain_h, w_up, w_down,
    out,
    lat, key_a, key_b, val_a, val_b, att, rows, goa, gob,
    gup, gdown, x, hid, act, res, even, odd, sib, part, land, table,
    stream, q_a, q_b, lat_gain, gain_a, gain_b, wk_a, wv_a, wk_b, wv_b, wo_a, wo_b, norm_gain,
    lat_s, lat_r, latf_s, latf_r, oa_s, oa_r, ob_s, ob_r,
    up_s, up_r, dn_s, dn_r, at_s, at_r, x_s, x_r, rs_s, rs_r, loc,
):
    s = lax.axis_index("sp")
    t = lax.axis_index("tp")
    core = t & 1
    length = q_a.shape[1]
    own = stream.shape[0]
    prow = lat.shape[1]
    half_rows = prow // 2
    depth_a = NOPE_A + ROPE
    depth_b = NOPE_B + ROPE
    heads_a = wk_a.shape[0] // NOPE_A
    heads_b = wk_b.shape[1] // NOPE_B
    hidden = gup.shape[2]
    wrows = w_up.shape[0]
    wcols = w_down.shape[1]
    features = stream.shape[1]
    width_a = heads_a * V_A
    width_b = heads_b * V_B
    start_b = att.shape[2] - width_b
    quarter = n // 4
    per = n // 8
    zone = s // quarter
    inner = (zone ^ (zone // 2)) & 1
    near = list(range(2, 2 * quarter, 2))
    first_far = (2 + inner) * quarter
    last_far = (3 - inner) * quarter
    up_half = wrows // 2
    cuts = 2 if wcols % 256 == 0 else 1
    cut = wcols // cuts

    def every(start, fn):
        if per == 1:
            fn(start)
        else:
            def step(j, carry):
                fn(start + 2 * j)
                return carry
            lax.fori_loop(0, per, step, 0)

    def copy(src, dst, ssem, rsem, sp, tp):
        return pltpu.make_async_remote_copy(
            src_ref=src, dst_ref=dst, send_sem=ssem, recv_sem=rsem,
            device_id={"sp": sp, "tp": tp}, device_id_type=pl.DeviceIdType.MESH,
        )

    barrier = pltpu.get_barrier_semaphore()

    def greet(sp, tp):
        pl.semaphore_signal(barrier, inc=1, device_id={"sp": sp, "tp": tp},
                            device_id_type=pl.DeviceIdType.MESH)

    for k in range(1, n):
        greet(s ^ k, t)
    for k in range(1, m):
        greet(s, t ^ k)
    greet(s ^ 2, t ^ 2)

    def halves(target):
        return pl.ds(pl.multiple_of(((target // 2) % 2) * hidden, 128), hidden)

    locals_ = [
        pltpu.make_async_copy(latent, lat.at[0, pl.ds(0, length)], loc.at[0]),
        pltpu.make_async_copy(rotary_t, lat.at[0, pl.ds(length, prow - length)], loc.at[1]),
        pltpu.make_async_copy(table_h, table, loc.at[2]),
        pltpu.make_async_copy(w_up.at[:, halves(s)], gup.at[0], loc.at[3]),
        pltpu.make_async_copy(w_down.at[halves(s)], gdown.at[0], loc.at[4]),
    ]
    early = [pltpu.make_async_copy(a, b, loc.at[5 + i]) for i, (a, b) in enumerate((
        (lat_gain_h, lat_gain), (gain_a_h, gain_a), (gain_b_h, gain_b), (wk_a_h, wk_a),
        (wv_a_h, wv_a), (wk_b_h, wk_b), (wv_b_h, wv_b)))]
    later = [pltpu.make_async_copy(a, b, loc.at[12 + i]) for i, (a, b) in enumerate((
        (q_a_h, q_a), (q_b_h, q_b), (wo_a_h, wo_a), (wo_b_h, wo_b), (stream_h, stream),
        (norm_gain_h, norm_gain)))]
    for c in locals_[:2] + early + locals_[2:] + later:
        c.start()
    locals_[0].wait()
    locals_[1].wait()
    pl.semaphore_wait(barrier, n + m - 1)

    mine = pl.ds(pl.multiple_of(core * half_rows, 16), half_rows)
    other = pl.ds(pl.multiple_of((1 - core) * half_rows, 16), half_rows)

    def lat_direct(k):
        return copy(lat.at[0, mine], lat.at[k, mine], lat_s.at[0], lat_r.at[k], s ^ k, t)

    def lat_across(k):
        return copy(lat.at[k, mine], lat.at[k + 1, mine], lat_s.at[0], lat_r.at[k + 1], s ^ 1, t)

    def lat_sibling(k):
        return copy(lat.at[k, mine], lat.at[k, mine], latf_s.at[0], latf_r.at[k], s, t ^ 1)

    def up_piece(k, r):
        at = pl.ds(r * up_half, up_half)
        return copy(w_up.at[at, halves(s ^ k)], gup.at[k, at], up_s.at[0],
                    up_r.at[2 * k + r], s ^ k, t)

    def up_across(k, r):
        at = pl.ds(r * up_half, up_half)
        return copy(gup.at[k, at], gup.at[k + 1, at], up_s.at[0],
                    up_r.at[2 * k + 2 + r], s ^ 1, t)

    def down_parts(k, h):
        at = pl.ds(h * cut, cut)
        size = hidden // (1 + h)
        for r in range(1 + h):
            yield (pl.ds(pl.multiple_of(((s ^ k) // 2) % 2 * hidden + r * size, 128), size),
                   pl.ds(r * size, size), at, h + r)

    def down_piece(k, h):
        return Several([
            copy(w_down.at[src, at], gdown.at[k, dst, at], dn_s.at[0], dn_r.at[3 * k + i], s ^ k, t)
            for src, dst, at, i in down_parts(k, h)])

    def down_across(k, h):
        return Several([
            copy(gdown.at[k, dst, at], gdown.at[k + 1, dst, at], dn_s.at[0],
                 dn_r.at[3 * k + 3 + i], s ^ 1, t)
            for src, dst, at, i in down_parts(k, h)])

    def up_send(k):
        for r in range(2):
            up_piece(k, r).start()

    def down_send(k):
        for h in range(cuts):
            down_piece(k, h).start()

    def up_on(k):
        for r in range(2):
            up_piece(k, r).wait_recv()
            up_across(k, r).start()

    def up_arrived(k):
        for r in range(2):
            up_piece(k, r).wait_recv()

    def down_on(k, h):
        for come, go in zip(down_piece(k, h).parts, down_across(k, h).parts):
            come.wait_recv()
            go.start()

    def downs_on(k):
        for h in range(cuts):
            down_on(k, h)

    def outer_only(fn):
        pl.when(inner == 0)(fn)

    def inner_only(fn):
        pl.when(inner == 1)(fn)

    lat_direct(1).start()
    for k in near:
        lat_direct(k).start()
    every(first_far, lambda k: lat_direct(k).start())
    every(last_far, lambda k: lat_direct(k).start())
    up_piece(1, 0).start()

    def out_a(k, slot):
        return copy(wo_a_h, goa.at[slot], oa_s.at[0], oa_r.at[slot], s, t ^ k)

    def out_b(k, slot):
        return copy(wo_b_h, gob.at[slot], ob_s.at[0], ob_r.at[slot], s, t ^ k)

    for k in (2, 1):
        out_a(k, k - 1).start()
        out_b(k, k - 1).start()

    @inner_only
    def _():
        every(last_far, up_send)
        every(first_far, up_send)
        for h in range(cuts):
            every(last_far, lambda k: down_piece(k, h).start())
            every(first_far, lambda k: down_piece(k, h).start())
        for k in near:
            up_send(k)

    @outer_only
    def _():
        for k in near:
            up_send(k)
        every(first_far, up_send)
        every(last_far, up_send)

    def make_block(k):
        source = lat.at[k]
        at = pl.ds(pl.multiple_of(k * length, length), length)
        wide = source[0:length, :].astype(F32)
        normed = (wide * lax.rsqrt(jnp.mean(wide * wide, axis=-1, keepdims=True) + EPSILON)
                  * lat_gain[...]).astype(BF16)
        rotary = source[length:prow, :].astype(F32).T
        squares = jnp.sum(rotary * rotary, axis=-1, keepdims=True)
        half = ROPE // 2
        turn = table[s ^ k]
        cosine = jnp.concatenate([turn[:, :half], turn[:, :half]], axis=-1)
        sine = jnp.concatenate([-turn[:, half:], turn[:, half:]], axis=-1)

        def turned(w):
            return lax.dot_general(normed, w[...], (((1,), (1,)), ((), ())),
                                   preferred_element_type=F32)

        def keys(flat, gain, nope, heads, dest):
            flat = flat.astype(BF16).astype(F32)
            for h in range(heads):
                piece = flat[:, h * nope:(h + 1) * nope]
                mean = (jnp.sum(piece * piece, axis=-1, keepdims=True) + squares) / (nope + ROPE)
                scale = lax.rsqrt(mean + EPSILON)
                dest[h, at, 0:nope] = (piece * scale * gain[:, 0:nope]).astype(BF16)
                last = rotary * scale * gain[:, nope:nope + ROPE]
                swapped = jnp.concatenate([last[:, half:], last[:, :half]], axis=-1)
                dest[h, at, nope:nope + ROPE] = (
                    last * cosine + swapped * sine).astype(BF16)

        keys(turned(wk_a), gain_a, NOPE_A, heads_a, key_a)
        keys(jnp.dot(normed, wk_b[...], preferred_element_type=F32), gain_b, NOPE_B, heads_b, key_b)
        val_a[at, :] = turned(wv_a).astype(BF16)
        val_b[at, :] = jnp.dot(normed, wv_b[...], preferred_element_type=F32).astype(BF16)

    locals_[2].wait()
    for c in early:
        c.wait()
    make_block(0)

    def arrived(k):
        lat_direct(k).wait_recv()

    def joined(k):
        copy(lat.at[k, other], lat.at[k, other], latf_s.at[0], latf_r.at[k], s, t ^ 1).wait_recv()
        make_block(k)

    def passed(k):
        arrived(k)
        lat_across(k).start()
        lat_sibling(k).start()

    def taken(k):
        arrived(k)
        lat_sibling(k).start()

    taken(1)
    for k in near:
        passed(k)
    every(first_far, passed)
    joined(1)
    every(last_far, passed)
    up_piece(1, 1).start()
    down_send(1)
    for k in near:
        joined(k)
    for k in near:
        taken(k + 1)
    every(first_far, joined)
    every(first_far + 1, taken)
    every(last_far, joined)
    every(last_far + 1, taken)
    for k in near:
        joined(k + 1)
    every(first_far + 1, joined)
    every(last_far + 1, joined)

    total = n * length
    block = min(total, 2048)
    number = total // block

    def attend(q, key, value, h, depth, width):
        query = q[h * depth:(h + 1) * depth, :].T

        def step(i, state):
            peak, sums, acc = state
            at = pl.ds(pl.multiple_of(i * block, block), block)
            score = lax.dot_general(query, key[h, at, :], (((1,), (1,)), ((), ())),
                                    preferred_element_type=F32) * depth ** (-0.5)
            new = jnp.maximum(peak, jnp.max(score, axis=-1, keepdims=True))
            shifted = jnp.exp(score - new)
            factor = jnp.exp(peak - new)
            sums = sums * factor + jnp.sum(shifted, axis=-1, keepdims=True)
            acc = acc * factor + jnp.dot(
                shifted.astype(BF16), value[at, h * width:(h + 1) * width],
                preferred_element_type=F32)
            return new, sums, acc

        state = (jnp.full((length, 1), -jnp.inf, F32), jnp.zeros((length, 1), F32),
                 jnp.zeros((length, width), F32))
        if number == 1:
            state = step(0, state)
        else:
            state = lax.fori_loop(0, number, step, state)
        return (state[2] / state[1]).astype(BF16)

    for c in later:
        c.wait()
    for h in range(heads_a):
        res_a = attend(q_a, key_a, val_a, h, depth_a, V_A)
        for j in range(m):
            att[j, :, h * V_A:(h + 1) * V_A] = res_a[j * own:(j + 1) * own]
    @inner_only
    def _():
        for k in near:
            up_on(k)

    for h in range(heads_b):
        res_b = attend(q_b, key_b, val_b, h, depth_b, V_B)
        for j in range(m):
            att[j, :, start_b + h * V_B:start_b + (h + 1) * V_B] = res_b[j * own:(j + 1) * own]

    def row_copy(k):
        return copy(att.at[t ^ k], rows.at[k], at_s.at[0], at_r.at[k], s, t ^ k)

    for k in (2, 3, 1):
        row_copy(k).start()

    def out_on_a():
        return copy(goa.at[1], goa.at[2], oa_s.at[0], oa_r.at[2], s, t ^ 1)

    def out_on_b():
        return copy(gob.at[1], gob.at[2], ob_s.at[0], ob_r.at[2], s, t ^ 1)

    def project(k, slot):
        return (jnp.dot(rows[k, :, 0:width_a], goa[slot], preferred_element_type=F32)
                + jnp.dot(rows[k, :, start_b:], gob[slot], preferred_element_type=F32))

    @outer_only
    def _():
        for k in near:
            up_on(k)

    inner_only(lambda: every(2 * quarter, up_on))
    mixed = (jnp.dot(att[t, :, 0:width_a], wo_a[...], preferred_element_type=F32)
             + jnp.dot(att[t, :, start_b:], wo_b[...], preferred_element_type=F32))
    out_a(1, 0).wait_recv()
    out_b(1, 0).wait_recv()
    row_copy(1).wait_recv()
    mixed += project(1, 0)
    out_a(2, 1).wait_recv()
    out_on_a().start()
    out_b(2, 1).wait_recv()
    out_on_b().start()
    row_copy(2).wait_recv()
    mixed += project(2, 1)
    out_on_a().wait_recv()
    out_on_b().wait_recv()
    row_copy(3).wait_recv()
    mixed += project(3, 2)
    residual = (stream[...].astype(F32) + mixed).astype(BF16)
    res[...] = residual
    wide = residual.astype(F32)
    x[0:own, :] = (wide * lax.rsqrt(jnp.mean(wide * wide, axis=-1, keepdims=True) + EPSILON)
                   * norm_gain[...]).astype(BF16)

    def peer(code):
        return (s ^ 2 if code & 4 else s), t ^ (code & 3)

    bit = own // 2

    def xcopy(src, dst, code):
        return Several([
            copy(x.at[pl.ds(src * own + i * bit, bit)], x.at[pl.ds(dst * own + i * bit, bit)],
                 x_s.at[0], x_r.at[2 * dst + i], *peer(code)) for i in range(2)])

    def xrelay():
        for i in range(2):
            xcopy(0, 4, 4).parts[i].wait_recv()
            xcopy(4, 6, 2).parts[i].start()
            xcopy(4, 5, 1).parts[i].start()

    xcopy(0, 4, 4).start()
    xcopy(0, 2, 2).start()
    xcopy(0, 1, 1).start()

    for k in near:
        down_send(k)

    @outer_only
    def _():
        for h in range(cuts):
            every(first_far, lambda k: down_piece(k, h).start())
            every(last_far, lambda k: down_piece(k, h).start())

    @outer_only
    def _():
        every(3 * quarter, up_on)
        every(2 * quarter, up_on)

    xcopy(0, 2, 2).wait_recv()
    xcopy(2, 3, 1).start()
    xrelay()
    inner_only(lambda: every(3 * quarter, up_on))
    xcopy(4, 6, 2).wait_recv()
    xcopy(6, 7, 1).start()
    for k in near:
        downs_on(k)

    def columns(k, size):
        return pl.ds(pl.multiple_of((s ^ k) * size, 128), size)

    def up(k):
        hid[...] += jnp.dot(x[:, columns(k, wrows)], gup[k], preferred_element_type=F32)

    def up_pair(k):
        up(k)
        up_arrived(k + 1)
        up(k + 1)

    for k in (1, 3, 5, 7):
        xcopy(k - 1, k, 1).wait_recv()
    locals_[3].wait()
    locals_[4].wait()
    hid[...] = jnp.dot(x[:, columns(0, wrows)], gup[0], preferred_element_type=F32)
    up_arrived(1)
    up(1)
    for k in near:
        up_pair(k)
    every(2 * quarter, up_pair)
    every(3 * quarter, up_pair)
    act[...] = jnp.square(jnp.maximum(hid[...], 0.0)).astype(BF16)

    def down(unit, k, h, width):
        base = ((s ^ k) % quarter) * width
        at = pl.ds(pl.multiple_of(base, 128), width)
        first = 0 if h is None else h * cut
        piece = jnp.dot(act[...], gdown[k, :, first:first + width], preferred_element_type=F32)
        for i in range(4):
            even[unit, i, :, at] = piece[2 * i * own:(2 * i + 1) * own]
            odd[unit, i, :, at] = piece[(2 * i + 1) * own:(2 * i + 2) * own].astype(BF16)

    def down_arrived(k):
        for h in range(cuts):
            down_piece(k, h).wait_recv()

    def down_pair(unit):
        def fn(k):
            down(unit, k, None, wcols)
            down_arrived(k + 1)
            down(unit, k + 1, None, wcols)
        return fn

    full = quarter * wcols
    mine_u = zone & 1
    next_u = 1 - mine_u
    places = ((2, s, t ^ 2), (4, s ^ 2, t), (6, s ^ 2, t ^ 2))

    def share(unit, width):
        return copy(odd.at[unit, :, :, 0:width], sib.at[unit, :, :, 0:width],
                    rs_s.at[0], rs_r.at[4 * unit], s, t ^ 1)

    def deliver(unit, width, i):
        _, sp, tp = places[i]
        return copy(part.at[unit, i, :, 0:width], land.at[unit, i, :, 0:width],
                    rs_s.at[0], rs_r.at[4 * unit + 1 + i], sp, tp)

    def scatter(unit, width):
        share(unit, width).wait_recv()
        for i in (2, 1, 0):
            part[unit, i, :, 0:width] = (even[unit, i + 1, :, 0:width]
                                         + sib[unit, i + 1, :, 0:width].astype(F32)).astype(BF16)
            deliver(unit, width, i).start()
        even[unit, 0, :, 0:width] += sib[unit, 0, :, 0:width].astype(F32)

    def finish(unit, width, group, h):
        for i in range(3):
            deliver(unit, width, i).wait_recv()
        base = (zone ^ group) * full
        spans = [(0, 0, full)] if h is None or cuts == 1 else [
            (j * cut, j * wcols + h * cut, cut) for j in range(quarter)]
        for lo, to, size in spans:
            at = pl.ds(pl.multiple_of(base + to, 128), size)
            out[:, at] = (res[:, at].astype(F32) + even[unit, 0, :, lo:lo + size]
                          + land[unit, 0, :, lo:lo + size].astype(F32)
                          + land[unit, 1, :, lo:lo + size].astype(F32)
                          + land[unit, 2, :, lo:lo + size].astype(F32)).astype(BF16)

    narrow = quarter * cut

    def far_unit(group, h):
        return 2 + cuts * ((zone ^ group) & 1) + h

    def far(group, h):
        start = group * quarter
        unit = far_unit(group, h)
        every(start, lambda k: down(unit, k, h, cut))
        every(start + 1, lambda k: down_piece(k, h).wait_recv())
        every(start + 1, lambda k: down(unit, k, h, cut))
        share(unit, narrow).start()

    def far_on(group, h):
        every(group * quarter, lambda k: down_on(k, h))

    down(mine_u, 0, None, wcols)
    down_arrived(1)
    down(mine_u, 1, None, wcols)
    for k in near:
        if k < quarter:
            down_pair(mine_u)(k)
    share(mine_u, full).start()
    one, two = 2 + inner, 3 - inner
    outer_only(lambda: far_on(one, 0))
    far_on(two, 0)
    for k in near:
        if k >= quarter:
            down_pair(next_u)(k)
    share(next_u, full).start()
    scatter(mine_u, full)

    @inner_only
    def _():
        if cuts > 1:
            far_on(two, 1)
        far_on(one, 0)

    far(2, 0)
    if cuts > 1:
        outer_only(lambda: far_on(two, 1))
    scatter(next_u, full)
    far(3, 0)
    scatter(far_unit(2, 0), narrow)
    if cuts > 1:
        far_on(one, 1)
        scatter(far_unit(3, 0), narrow)
        far(two, 1)
        scatter(far_unit(two, 1), narrow)
        far(one, 1)
        scatter(far_unit(one, 1), narrow)
        finish(mine_u, full, 0, None)
        finish(next_u, full, 1, None)
    else:
        scatter(far_unit(3, 0), narrow)
        finish(mine_u, full, 0, None)
        finish(next_u, full, 1, None)
    for group in (two, one):
        for h in range(cuts):
            finish(far_unit(group, h), narrow, group, h)

    def drained(ref, sem):
        copy(ref, ref, sem.at[0], sem.at[0], s, t ^ 1).wait_send()

    drained(lat.at[pl.ds(1, n - 1), mine], lat_s)
    drained(lat.at[pl.ds(1, n - 1), mine], latf_s)
    drained(gup.at[pl.ds(1, n - 1)], up_s)
    drained(gdown.at[pl.ds(1, n - 1)], dn_s)
    drained(goa, oa_s)
    drained(gob, ob_s)
    drained(rows.at[pl.ds(1, m - 1)], at_s)
    drained(x.at[pl.ds(own, 7 * own)], x_s)
    drained(x.at[pl.ds(0, 7 * own)], rs_s)


def body(n, m, stream, query_a, query_b, latent, rotary_key, latent_gain, key_gain_a, key_gain_b,
         w_key_a, w_value_a, w_key_b, w_value_b, w_out_a, w_out_b, norm_gain, w_up, w_down):
    length, rank = latent.shape
    own, features = stream.shape
    half = ROPE // 2
    freqs = np.float32(THETA) ** (-np.arange(half, dtype=np.float32) / np.float32(half))
    angle = np.arange(n * length).astype(np.float32)[:, None] * freqs
    cosine, sine = np.cos(angle), np.sin(angle)
    table = jnp.asarray(np.concatenate([cosine, sine], axis=-1).reshape(n, length, ROPE))
    total = n * length
    heads_a = w_key_a.shape[1] // NOPE_A
    heads_b = w_key_b.shape[1] // NOPE_B
    width_a = -(-heads_a * V_A // 128) * 128
    width_b = heads_b * V_B
    hidden = w_up.shape[1] // 2
    V = pltpu.VMEM
    dma = lambda k: pltpu.SemaphoreType.DMA((k,))
    tokens = 2 * m * own
    group = features // 4
    units = 6 if w_down.shape[1] % 256 == 0 else 4
    scratch = [
        V((n, length + ROPE, rank), BF16),
        V((heads_a, total, NOPE_A + ROPE), BF16),
        V((heads_b, total, NOPE_B + ROPE), BF16),
        V((total, heads_a * V_A), BF16),
        V((total, heads_b * V_B), BF16),
        V((m, own, width_a + width_b), BF16),
        V((m, own, width_a + width_b), BF16),
        V((m - 1,) + w_out_a.shape, BF16),
        V((m - 1,) + w_out_b.shape, BF16),
        V((n, w_up.shape[0], hidden), BF16),
        V((n, hidden, w_down.shape[1]), BF16),
        V((tokens, features), BF16),
        V((tokens, hidden), F32),
        V((tokens, hidden), BF16),
        V((own, features), BF16),
        V((units, 4, own, group), F32),
        V((units, 4, own, group), BF16),
        V((units, 4, own, group), BF16),
        V((units, 3, own, group), BF16),
        V((units, 3, own, group), BF16),
        V(table.shape, F32),
    ]
    given = (stream, query_a.T, query_b.T, latent_gain[None], key_gain_a[None], key_gain_b[None],
             w_key_a.T, w_value_a.T, w_key_b, w_value_b, w_out_a, w_out_b, norm_gain[None])
    scratch += [V(a.shape, a.dtype) for a in given]
    sizes = [1, n, 1, n, 1, 3, 1, 3, 1, 2 * n, 1, 3 * n, 1, m, 1, 16, 1, 24, 18]
    scratch += [dma(k) for k in sizes]
    vmem = pl.BlockSpec(memory_space=V)
    hbm = pl.BlockSpec(memory_space=pl.ANY)
    return pl.pallas_call(
        functools.partial(kernel, n, m),
        out_shape=jax.ShapeDtypeStruct((own, features), BF16),
        in_specs=[hbm] * 18,
        out_specs=vmem,
        scratch_shapes=scratch,
        compiler_params=pltpu.CompilerParams(
            collective_id=0, has_side_effects=True, vmem_limit_bytes=67043328),
        name="layer",
    )(stream, query_a.T, query_b.T, latent, rotary_key.T, table, latent_gain[None], key_gain_a[None],
      key_gain_b[None], w_key_a.T, w_value_a.T, w_key_b, w_value_b, w_out_a, w_out_b,
      norm_gain[None], w_up, w_down)


def solution(mesh):
    n, m = mesh.shape["sp"], mesh.shape["tp"]
    in_specs = (
        P(("sp", "tp"), None),
        P("sp", "tp"),
        P("sp", "tp"),
        P("sp", None),
        P("sp", None),
        P(),
        P(),
        P(),
        P(None, "tp"),
        P(None, "tp"),
        P(None, "tp"),
        P(None, "tp"),
        P("tp", None),
        P("tp", None),
        P(),
        P("sp", "tp"),
        P("tp", "sp"),
    )
    out_specs = P(("sp", "tp"), None)
    return jax.shard_map(functools.partial(body, n, m), mesh=mesh, in_specs=in_specs,
                         out_specs=out_specs, check_vma=False)
```
